128 devices in a mesh: ep: 32 (over z, y, core), tp: 4 (over x).
Axes of the slice: x: 4, y: 4, z: 4, core: 2. Of those that a mesh axis runs over, the one named last changes fastest.
Arguments:
- mixer_microbatch: bfloat16 [32768, 2048], P(('ep', 'tp')), may hold values from -6 to 6
- mixer_gain_vector: float32 [2048], replicated, may hold values from 0.1 to 1.9
- asker_matrix: bfloat16 [2048, 1024], P(None, 'tp'), may hold values from -0.125 to 0.125
- matcher_matrix: bfloat16 [2048, 1024], P(None, 'tp'), may hold values from -0.125 to 0.125
- fading_matrix: bfloat16 [2048, 1024], P(None, 'tp'), may hold values from -0.125 to 0.125
- content_matrix: bfloat16 [2048, 2048], P(None, 'tp'), may hold values from -0.125 to 0.125
- result_valve_matrix: bfloat16 [2048, 2048], P(None, 'tp'), may hold values from -0.125 to 0.125
- fading_shift_vector: float32 [1024], P('tp'), may hold values from -1.5 to 20
- extra_fade_amount: float32 [32768, 16], P('ep', 'tp'), may hold values from -0.7 to 0
- starting_memory: float32 [1024, 128], P('tp'), may hold values from -24 to 24
- subspace_gain_vector: float32 [2048], P('tp'), may hold values from 0.1 to 1.9
- result_matrix: bfloat16 [2048, 2048], replicated, may hold values from -0.125 to 0.125
- specialist_microbatch: bfloat16 [16384, 2048], P(('ep', 'tp')), may hold values from -6 to 6
- specialist_gain_vector: float32 [2048], replicated, may hold values from 0.1 to 1.9
- picked_specialists: int32 [16384, 2], P(('ep', 'tp')), may hold values from 0 to 63, all different within a row; in each aligned block of 128 rows (0 to 127, 128 to 255, ...) at most 6 rows name the same one
- specialist_mixing_factor: float32 [16384, 2], P(('ep', 'tp')), may hold values from 0.3 to 1.5
- specialist_valve_matrix: bfloat16 [64, 2048, 1024], P('ep', None, 'tp'), may hold values from -0.125 to 0.125
- specialist_widen_matrix: bfloat16 [64, 2048, 1024], P('ep', None, 'tp'), may hold values from -0.125 to 0.125
- specialist_shrink_matrix: bfloat16 [64, 1024, 2048], P('ep', 'tp'), may hold values from -0.1875 to 0.1875
- joint_valve_matrix: bfloat16 [2048, 512], P(None, 'tp'), may hold values from -0.125 to 0.125
- joint_widen_matrix: bfloat16 [2048, 512], P(None, 'tp'), may hold values from -0.125 to 0.125
- joint_shrink_matrix: bfloat16 [512, 2048], P('tp'), may hold values from -0.25 to 0.25
Outputs:
- mixer_sublayer_result: bfloat16 [32768, 2048], P(('ep', 'tp'))
- moe_out: bfloat16 [16384, 2048], P(('ep', 'tp'))
The draws below stay inside these ranges and needn't reach their ends.
Inputs may be any that keep to these rules, and one draw needn't show every extreme that they name: `picked_specialists`: each row names 2 different experts; among the rows of one device no expert is named more than 6 times.
All inputs are finite; a program needn't handle non-finite values.
Results may differ from the reference program's by a relative error of at most 0.025.
Values may be sent and summed in bfloat16 or wider, within the bound.
A program may use at most 192 MiB of HBM per device.

```python
import math
import jax
import jax.numpy as jnp
import numpy as np
from jax import lax

D = 2048
NUM_SUBSPACES = 16
MATCHER_WIDTH = 64
DV = 128
SPAN_LENGTH = 64
TOK_MOE = 128
TOP_K = 2
FFE = 1024
FFS = 512
EXPERTS = 64
CAP = 6
TOKENS_A = 32768
TOKENS_B = 16384
N_EP = 32
N_TP = 4


def draw_fading_shift_vector(key, part):
    key_one, key_two, key_three = jax.random.split(jax.random.fold_in(key, 11), 3)
    shuffled = jax.random.permutation(key_one, NUM_SUBSPACES)
    fast_head = shuffled < NUM_SUBSPACES // 2
    slow_value = jnp.log(jnp.float32(TOKENS_A) * 0.206)
    fast_value = jax.random.uniform(key_two, (NUM_SUBSPACES, MATCHER_WIDTH), jnp.float32, -1.0, 0.5)
    jitter = jax.random.uniform(key_three, (NUM_SUBSPACES, MATCHER_WIDTH), jnp.float32, -0.5, 0.5)
    result_value = jnp.where(fast_head[:, None], fast_value, slow_value + jitter)
    return result_value.reshape(NUM_SUBSPACES * MATCHER_WIDTH).astype(jnp.float32)


def draw_extra_fade_amount(key, part):
    key_one, key_two = jax.random.split(jax.random.fold_in(key, 23), 2)
    where_rows = jax.random.randint(key_one, (3,), 0, TOKENS_A)
    drop_depth = jnp.log(jax.random.uniform(key_two, (3, NUM_SUBSPACES), jnp.float32, 0.5, 0.8))
    positions = jnp.arange(TOKENS_A, dtype=jnp.int32)
    matches = (positions[:, None] == where_rows[None, :]).astype(jnp.float32)
    return jnp.dot(matches, drop_depth, precision=lax.Precision.HIGHEST)


def block_scale(rng, extent, cuts, least, largest):
    factor_of = 1.0
    for axis_at, parts in cuts:
        steps = jax.random.uniform(jax.random.fold_in(jax.random.fold_in(rng, 6), axis_at), (parts,), jnp.float32, least / len(cuts), largest / len(cuts))
        factor_of = factor_of * jnp.repeat(jnp.exp(steps), extent[axis_at] // parts).reshape((-1,) + (1,) * (len(extent) - 1 - axis_at))
    return factor_of


def shared_out(key, own, number, rows, amount, top, limit, slope):
    ranking = jax.random.permutation(key, amount)
    packed, ordinary = portions_of(amount, rows * top, limit, slope, True), portions_of(amount, rows * top, limit, slope, False)
    places = jnp.arange(amount)

    def named(sizes, offset_by):
        used = int((sizes > 0).sum())
        fixed = max(1, used // 4)
        moved = fixed + (places - fixed + offset_by * (used - fixed)) % max(1, amount - fixed)
        return jnp.zeros((amount,), jnp.int32).at[ranking[jnp.where(places < fixed, places, moved)]].set(jnp.asarray(sizes, jnp.int32))

    sizes = jnp.where(number % 4 == 0, named(packed, number // 4), named(ordinary, number - number // 4 - 1))
    mixed = jax.random.permutation(jax.random.fold_in(own, 3), amount)
    giver, receiver = mixed[0:amount // 2 * 2:2], mixed[1:amount // 2 * 2:2]
    margin = jnp.minimum(sizes[giver] - 1, limit - sizes[receiver]) // 2
    margin = jnp.where((giver == ranking[0]) | (receiver == ranking[0]) | (sizes[receiver] == 0), 0, jnp.maximum(margin, 0))
    moved = jax.random.randint(jax.random.fold_in(own, 4), (amount // 2,), 0, 1 << 20) % (margin + 1)
    sizes = sizes.at[giver].add(-moved).at[receiver].add(moved)
    members = jnp.searchsorted(jnp.cumsum(sizes), jnp.arange(rows * top), side="right").astype(jnp.int32)
    listing = members.reshape(top, rows).T
    listing = listing[jax.random.permutation(jax.random.fold_in(own, 1), rows)]
    offset_by = jax.random.randint(jax.random.fold_in(own, 2), (rows, 1), 0, top)
    return jnp.take_along_axis(listing, (jnp.arange(top)[None, :] + offset_by) % top, axis=1)


def portions_of(number_of, total, most, lean, full):
    portions = [(1 << 20) // math.isqrt(grade ** lean) + 1 for grade in range(1, number_of + 1)]
    largest = most if full else min(most, max(-(-total // number_of), total * portions[0] // sum(portions)))
    least = 1 if total - largest >= number_of - 1 else 0
    holding, spare = [largest] + [least] * (number_of - 1), total - largest - least * (number_of - 1)
    while spare > 0:
        free = [i for i in range(1, number_of) if holding[i] < largest] or [i for i in range(1, number_of) if holding[i] < most]
        mass, left = sum([portions[i] for i in free]), spare
        for i in free:
            more = min(most - holding[i], max(1, left * portions[i] // mass), spare)
            holding[i] = holding[i] + more
            spare = spare - more
    return np.array(holding)


def bell_draw(rng, dims, scale, limit, cuts=(), held_as=jnp.bfloat16):
    drawn = jax.random.normal(rng, dims, jnp.float32) * scale
    if len(cuts) > 0:
        drawn = block_scale(rng, dims, cuts, -0.22, 0.18) * drawn
    return jnp.clip(drawn, min=-limit, max=limit).astype(held_as)


def setup_inputs(seed: int = 0) -> dict:
    arg_keys = jax.random.split(jax.random.key(seed), 23)
    mixer_microbatch = bell_draw(arg_keys[0], (TOKENS_A, D), 1.0, 6.0, ((0, 128),))
    mixer_gain_vector = jnp.clip(1.0 + 0.18 * jax.random.normal(arg_keys[1], (D,), jnp.float32), 0.1, 1.9)
    asker_matrix = bell_draw(arg_keys[2], (D, NUM_SUBSPACES * MATCHER_WIDTH), D ** -0.5, 0.125, ((1, 4),))
    matcher_matrix = bell_draw(arg_keys[3], (D, NUM_SUBSPACES * MATCHER_WIDTH), D ** -0.5, 0.125, ((1, 4),))
    fading_matrix = bell_draw(arg_keys[4], (D, NUM_SUBSPACES * MATCHER_WIDTH), D ** -0.5, 0.125, ((1, 4),))
    content_matrix = bell_draw(arg_keys[5], (D, NUM_SUBSPACES * DV), D ** -0.5, 0.125, ((1, 4),))
    result_valve_matrix = bell_draw(arg_keys[6], (D, NUM_SUBSPACES * DV), D ** -0.5, 0.125, ((1, 4),))
    fading_shift_vector = draw_fading_shift_vector(jax.random.fold_in(arg_keys[22], 71), 0)
    extra_fade_amount = draw_extra_fade_amount(jax.random.fold_in(arg_keys[22], 71), 0)
    starting_memory = bell_draw(arg_keys[9], (NUM_SUBSPACES * MATCHER_WIDTH, DV), 4.0, 24.0, ((0, 4),), jnp.float32)
    subspace_gain_vector = jnp.clip(1.0 + 0.18 * jax.random.normal(arg_keys[10], (NUM_SUBSPACES * DV,), jnp.float32), 0.1, 1.9)
    result_matrix = bell_draw(arg_keys[11], (NUM_SUBSPACES * DV, D), (NUM_SUBSPACES * DV) ** -0.5, 0.125)
    specialist_microbatch = bell_draw(arg_keys[12], (TOKENS_B, D), 1.0, 6.0, ((0, 128),))
    specialist_gain_vector = jnp.clip(1.0 + 0.18 * jax.random.normal(arg_keys[13], (D,), jnp.float32), 0.1, 1.9)
    picked_specialists_keys = jax.random.split(jax.random.fold_in(arg_keys[14], 1), TOKENS_B // TOK_MOE)
    picked_specialists_turns = jax.random.permutation(jax.random.fold_in(arg_keys[14], 3), TOKENS_B // TOK_MOE)
    picked_specialists = jax.vmap(lambda own, number: shared_out(jax.random.fold_in(arg_keys[14], 2), own, number, TOK_MOE, EXPERTS, TOP_K, CAP, 1))(picked_specialists_keys, picked_specialists_turns).reshape((TOKENS_B, TOP_K))
    specialist_mixing_factor = jnp.clip(jnp.exp(math.log(1.5) - 1.60943787 * jax.random.uniform(arg_keys[15], (TOKENS_B, TOP_K), jnp.float32) ** block_scale(arg_keys[15], (TOKENS_B, TOP_K), ((0, 128),), -0.2, 0.2)), 0.3, 1.5)
    specialist_valve_matrix = bell_draw(arg_keys[16], (EXPERTS, D, FFE), D ** -0.5, 0.125, ((0, 32), (2, 4)))
    specialist_widen_matrix = bell_draw(arg_keys[17], (EXPERTS, D, FFE), D ** -0.5, 0.125, ((0, 32), (2, 4)))
    specialist_shrink_matrix = bell_draw(arg_keys[18], (EXPERTS, FFE, D), FFE ** -0.5, 0.1875, ((0, 32), (1, 4)))
    joint_valve_matrix = bell_draw(arg_keys[19], (D, FFS), D ** -0.5, 0.125, ((1, 4),))
    joint_widen_matrix = bell_draw(arg_keys[20], (D, FFS), D ** -0.5, 0.125, ((1, 4),))
    joint_shrink_matrix = bell_draw(arg_keys[21], (FFS, D), FFS ** -0.5, 0.25, ((0, 4),))
    return dict(mixer_microbatch=mixer_microbatch, mixer_gain_vector=mixer_gain_vector, asker_matrix=asker_matrix, matcher_matrix=matcher_matrix, fading_matrix=fading_matrix, content_matrix=content_matrix, result_valve_matrix=result_valve_matrix, fading_shift_vector=fading_shift_vector, extra_fade_amount=extra_fade_amount, starting_memory=starting_memory, subspace_gain_vector=subspace_gain_vector, result_matrix=result_matrix, specialist_microbatch=specialist_microbatch, specialist_gain_vector=specialist_gain_vector, picked_specialists=picked_specialists, specialist_mixing_factor=specialist_mixing_factor, specialist_valve_matrix=specialist_valve_matrix, specialist_widen_matrix=specialist_widen_matrix, specialist_shrink_matrix=specialist_shrink_matrix, joint_valve_matrix=joint_valve_matrix, joint_widen_matrix=joint_widen_matrix, joint_shrink_matrix=joint_shrink_matrix)


NORM_EPS = 1e-06
GATE_SOFTNESS = 16.0
exact_precision = lax.Precision.HIGHEST

def rms_rows(values, gain):
    widened = values.astype(jnp.float32)
    inverse_rms = lax.rsqrt(lax.optimization_barrier(jnp.mean(widened * widened, axis=-1, keepdims=True)) + NORM_EPS)
    return (widened * inverse_rms * gain).astype(jnp.bfloat16)

def expert_apply(rows_in, gate_w, up_w, down_w):
    gate_value = jnp.dot(rows_in, gate_w, preferred_element_type=jnp.float32)
    up_value = jnp.dot(rows_in, up_w, preferred_element_type=jnp.float32)
    hidden = (jax.nn.silu(gate_value) * up_value).astype(jnp.bfloat16)
    group_width = down_w.shape[0] // N_TP
    combined = jnp.zeros((rows_in.shape[0], down_w.shape[1]), jnp.float32)
    for group_index in range(N_TP):
        row_lower = group_index * group_width
        partial_sum = jnp.dot(hidden[:, row_lower:row_lower + group_width], down_w[row_lower:row_lower + group_width], preferred_element_type=jnp.float32)
        rounded = lax.optimization_barrier(partial_sum.astype(jnp.bfloat16))
        combined = combined + rounded.astype(jnp.float32)
    return combined.astype(jnp.bfloat16)

def mixer_share(mixer_microbatch, mixer_gain_vector, asker_matrix, matcher_matrix, fading_matrix, content_matrix, result_valve_matrix, fading_shift_vector, extra_fade_amount, starting_memory, subspace_gain_vector, result_matrix):
    normed = rms_rows(mixer_microbatch, mixer_gain_vector)

    def project(weight):
        return jnp.dot(normed, weight, preferred_element_type=jnp.float32).astype(jnp.bfloat16)
    query, key_rows, decay_logits, value, gate_pre = (project(asker_matrix), project(matcher_matrix), project(fading_matrix), project(content_matrix), project(result_valve_matrix))
    logarithmic_fading_speed = jax.nn.log_sigmoid(decay_logits.astype(jnp.float32) + fading_shift_vector) / GATE_SOFTNESS
    span_sequence = TOKENS_A // SPAN_LENGTH
    dimension_signature = (span_sequence, SPAN_LENGTH, NUM_SUBSPACES, MATCHER_WIDTH)
    query_wide = query.astype(jnp.float32).reshape(dimension_signature) * MATCHER_WIDTH ** (-0.5)
    key_wide = key_rows.astype(jnp.float32).reshape(dimension_signature)
    value_wide = value.astype(jnp.float32).reshape(span_sequence, SPAN_LENGTH, NUM_SUBSPACES, DV)
    speed_expanded = logarithmic_fading_speed.reshape(dimension_signature) + extra_fade_amount.reshape(span_sequence, SPAN_LENGTH, NUM_SUBSPACES, 1)
    causal_mask = jnp.tril(jnp.ones((SPAN_LENGTH, SPAN_LENGTH), bool))

    def step(carried_state, inputs):
        query_block, key_block, block_values, rate_block = inputs
        running = jnp.cumsum(rate_block, axis=0)
        block_total = running[-1:]
        query_faded = query_block * jnp.exp(running)
        k_decayed = key_block * jnp.exp(-running)
        key_until_finish = key_block * jnp.exp(block_total - running)
        scores = jnp.einsum('ihk,jhk->hij', query_faded, k_decayed, precision=exact_precision)
        scores = jnp.where(causal_mask[None], scores, 0.0)
        inner_part = jnp.einsum('hij,jhv->ihv', scores, block_values, precision=exact_precision)
        outer_contribution = jnp.einsum('wzr,zrg->wzg', query_faded, carried_state, precision=exact_precision)
        added_terms = jnp.einsum('aqe,aqf->qef', key_until_finish, block_values, precision=exact_precision)
        updated = jnp.exp(block_total[0])[..., None] * carried_state + added_terms
        return (updated, inner_part + outer_contribution)
    first_state = starting_memory.astype(jnp.float32).reshape(NUM_SUBSPACES, MATCHER_WIDTH, DV)
    _, attended = lax.scan(step, first_state, (query_wide, key_wide, value_wide, speed_expanded))
    attended = attended.reshape(TOKENS_A, NUM_SUBSPACES, DV)
    inverse_rms = lax.rsqrt(lax.optimization_barrier(jnp.mean(attended * attended, axis=-1, keepdims=True)) + NORM_EPS)
    normed_heads = (attended * inverse_rms).reshape(TOKENS_A, NUM_SUBSPACES * DV) * subspace_gain_vector
    headed = (normed_heads * jax.nn.silu(gate_pre.astype(jnp.float32))).astype(jnp.bfloat16)
    return jnp.dot(headed, result_matrix, preferred_element_type=jnp.float32).astype(jnp.bfloat16)

def expert_half(specialist_microbatch, specialist_gain_vector, picked_specialists, specialist_mixing_factor, specialist_valve_matrix, specialist_widen_matrix, specialist_shrink_matrix, joint_valve_matrix, joint_widen_matrix, joint_shrink_matrix):
    normed = rms_rows(specialist_microbatch, specialist_gain_vector)
    devices = N_EP * N_TP
    flat_expert = picked_specialists.reshape(devices, TOK_MOE * TOP_K)
    matches = (flat_expert[..., None] == jnp.arange(EXPERTS, dtype=jnp.int32)).astype(jnp.int32)
    slot_rank = lax.optimization_barrier(jnp.sum(jnp.cumsum(matches, axis=1) * matches, axis=2)) - 1
    device_ids = jnp.arange(devices, dtype=jnp.int32)[:, None]
    column = device_ids * CAP + slot_rank
    token_ids = device_ids * TOK_MOE + jnp.arange(TOK_MOE * TOP_K, dtype=jnp.int32)[None, :] // TOP_K
    slot_table = jnp.full((EXPERTS, devices * CAP), TOKENS_B, jnp.int32).at[flat_expert, column].set(token_ids)
    padded = jnp.concatenate([normed, jnp.zeros((1, normed.shape[1]), jnp.bfloat16)], axis=0)

    def one_expert(expert_index):
        picked_rows = padded[slot_table[expert_index]]
        return expert_apply(picked_rows, specialist_valve_matrix[expert_index], specialist_widen_matrix[expert_index], specialist_shrink_matrix[expert_index])
    outputs = lax.map(one_expert, jnp.arange(EXPERTS, dtype=jnp.int32))
    picked = outputs[flat_expert, column].reshape(TOKENS_B, TOP_K, normed.shape[1])
    shared = expert_apply(normed, joint_valve_matrix, joint_widen_matrix, joint_shrink_matrix)
    combined = shared.astype(jnp.float32) + lax.optimization_barrier(jnp.sum(specialist_mixing_factor[:, :, None] * picked.astype(jnp.float32), axis=1))
    return combined.astype(jnp.bfloat16)

def reference(mixer_microbatch, mixer_gain_vector, asker_matrix, matcher_matrix, fading_matrix, content_matrix, result_valve_matrix, fading_shift_vector, extra_fade_amount, starting_memory, subspace_gain_vector, result_matrix, specialist_microbatch, specialist_gain_vector, picked_specialists, specialist_mixing_factor, specialist_valve_matrix, specialist_widen_matrix, specialist_shrink_matrix, joint_valve_matrix, joint_widen_matrix, joint_shrink_matrix):
    mixer_sublayer_result = mixer_share(mixer_microbatch, mixer_gain_vector, asker_matrix, matcher_matrix, fading_matrix, content_matrix, result_valve_matrix, fading_shift_vector, extra_fade_amount, starting_memory, subspace_gain_vector, result_matrix)
    moe_out = expert_half(specialist_microbatch, specialist_gain_vector, picked_specialists, specialist_mixing_factor, specialist_valve_matrix, specialist_widen_matrix, specialist_shrink_matrix, joint_valve_matrix, joint_widen_matrix, joint_shrink_matrix)
    return (mixer_sublayer_result, moe_out)
```

```python
import functools
import jax
import jax.numpy as jnp
from jax import lax
from jax.experimental import pallas as pl
from jax.experimental.pallas import tpu as pltpu
from jax.sharding import PartitionSpec as P

NORM_EPS = 1e-06
F32 = jnp.float32
BF16 = jnp.bfloat16
MESH = pl.DeviceIdType.MESH
EXACT = lax.Precision.HIGHEST
CHUNKS = 4
SPAN = 64


def rms(values, gain):
    wide = values.astype(F32)
    scale = lax.rsqrt(jnp.mean(wide * wide, axis=-1, keepdims=True) + NORM_EPS)
    return (wide * scale * gain).astype(BF16)


def at(start, size, unit=None):
    return pl.ds(pl.multiple_of(start, unit or size), size)


def layer_kernel(
    shape,
    xa_hbm, ga_ref, wq_hbm, wk_hbm, wf_hbm, wc_hbm, wg_hbm, shift_ref, fade_ref, first_ref,
    hgain_ref, wr_hbm,
    x_hbm, gain_ref, meta_ref, wv_hbm, wu_hbm, wd_hbm, jv_hbm, ju_hbm, jd_hbm,
    mix_out, moe_out,
    xa, na, wa, pj, att, qg, state, sent, heard, pt,
    x_ref, wv, wu, wd, jv, ju, jd,
    gm, metas, onehot, weigh, tx, rx, hid, ry, shid, fx,
    wsem, ags, agr, ms, mr, dts, drs, dls, rts, rrs, rls, fs, fr,
    aas, aar, ss, sr, hs, hr,
):
    n_ep, n_tp, tok, width, slots, ffe, seg, kw, vw = shape
    per = n_tp * 2 * slots
    rows = n_ep * per
    wc = width // CHUNKS
    part_rows = 512
    heads = vw // 128
    segrows = seg * n_tp
    quarter = seg // 4
    ep = lax.axis_index("ep")
    tp = lax.axis_index("tp")
    core, yy, zz = lax.rem(ep, 2), lax.rem(ep // 2, 4), ep // 8
    right = lax.rem(tp + 1, n_tp)
    left = lax.rem(tp + n_tp - 1, n_tp)
    across = lax.rem(tp + 2, n_tp)

    def peer(i):
        return (
            lax.rem(zz + i // 8, 4) * 8
            + lax.rem(yy + lax.rem(i // 2, 4), 4) * 2
            + lax.rem(core + lax.rem(i, 2), 2)
        )

    pairs = [
        (x_hbm, x_ref), (xa_hbm, xa),
        (wq_hbm, wa.at[:, 0:kw]), (wk_hbm, wa.at[:, kw : 2 * kw]), (wf_hbm, wa.at[:, 2 * kw : 3 * kw]),
        (wc_hbm, wa.at[:, 3 * kw : 3 * kw + vw]), (wg_hbm, wa.at[:, 3 * kw + vw : 3 * kw + 2 * vw]),
        (jv_hbm, jv), (ju_hbm, ju), (wv_hbm, wv), (wu_hbm, wu), (wd_hbm, wd), (jd_hbm, jd),
    ]
    loads = [pltpu.make_async_copy(s, d, wsem.at[i]) for i, (s, d) in enumerate(pairs)]
    for copy in loads:
        copy.start()

    barrier = pltpu.get_barrier_semaphore()

    def greet(i, carry):
        pl.semaphore_signal(barrier, inc=1, device_id={"ep": peer(i)}, device_id_type=MESH)
        return carry

    lax.fori_loop(1, n_ep, greet, 0)
    for step in range(1, n_tp):
        pl.semaphore_signal(
            barrier, inc=1, device_id={"tp": lax.rem(tp + step, n_tp)}, device_id_type=MESH
        )

    loads[0].wait()
    normed = rms(x_ref[...], gain_ref[...])
    mine = at(tp * tok, tok)
    for c in range(CHUNKS):
        gm[c, mine, :] = normed[:, c * wc : (c + 1) * wc]

    meta = meta_ref[...]
    tall = jnp.concatenate([meta, jnp.zeros((tok - 8, tok), F32)], axis=0).T
    before = lax.broadcasted_iota(jnp.int32, (tok, tok), 0) < lax.broadcasted_iota(
        jnp.int32, (tok, tok), 1
    )
    names = meta[0:2].astype(jnp.int32)
    tall_names = tall[:, 0:2].astype(jnp.int32)
    spots = []
    for k in range(2):
        row = names[k : k + 1]
        hits = jnp.zeros((tok, tok), F32)
        for j in range(2):
            hits = hits + jnp.where((tall_names[:, j : j + 1] == row) & before, 1.0, 0.0)
        rank = jnp.sum(hits, axis=0, keepdims=True)
        local = row // 2
        base = (local * per + tp * 2 * slots + (row - 2 * local) * slots).astype(F32)
        spots.append(base + rank)
    metas[at(tp * 8, 8), :] = jnp.concatenate(
        [spots[0], spots[1], meta[2:4], jnp.zeros((4, tok), F32)], axis=0
    )

    pl.semaphore_wait(barrier, n_ep - 1 + n_tp - 1)

    my_meta = metas.at[at(tp * 8, 8)]
    sends = []

    def send_tp(src, dst, ssem, rsem, to):
        copy = pltpu.make_async_remote_copy(
            src_ref=src, dst_ref=dst, send_sem=ssem, recv_sem=rsem,
            device_id={"tp": to}, device_id_type=MESH,
        )
        copy.start()
        sends.append(copy)

    def arrived(ref, sem):
        pltpu.make_async_copy(ref, ref, sem).wait()

    for step in range(1, n_tp):
        send_tp(my_meta, my_meta, ms.at[step], mr.at[step], lax.rem(tp + step, n_tp))

    def block(c, who, half=None):
        if half is None:
            return gm.at[c, at(who * tok, tok)]
        return gm.at[c, at(who * tok + half * (tok // 2), tok // 2)]

    for c in range(CHUNKS):
        own = block(c, tp)
        send_tp(own, own, ags.at[c, 0], agr.at[c, 0], right)
        send_tp(own, own, ags.at[c, 1], agr.at[c, 1], left)

    loads[1].wait()
    for i in range(4):
        r = slice(i * quarter, (i + 1) * quarter)
        na[at(tp * seg + i * quarter, quarter), :] = rms(xa[r, :], ga_ref[...])

    def ablock(who, i):
        return na.at[at(who * seg + i * quarter, quarter)]

    def attention_send(i):
        own = ablock(tp, i)
        send_tp(own, own, aas.at[0, i], aar.at[0, i], right)
        send_tp(own, own, aas.at[1, i], aar.at[1, i], left)

    for step in range(1, n_tp):
        arrived(metas.at[at(lax.rem(tp + n_tp - step, n_tp) * 8, 8)], mr.at[step])

    def table(t, carry):
        r0 = pl.multiple_of(t * 256, 256)
        ids = lax.broadcasted_iota(jnp.int32, (256, tok), 0) + r0
        for m in range(n_tp):
            spot = metas[8 * m : 8 * m + 2, :].astype(jnp.int32)
            hit = (ids == spot[0:1]) | (ids == spot[1:2])
            onehot[pl.ds(r0, 256), m * tok : (m + 1) * tok] = jnp.where(hit, 1.0, 0.0).astype(BF16)
        return carry

    lax.fori_loop(0, rows // 256, table, 0)

    def local_rows(c, src, dst, sem):
        own = at(ep * per, per)
        return pltpu.make_async_copy(src.at[c, own], dst.at[c, own], sem.at[c])

    def spread(c, src, dst, ssem, rsem):
        def one(i, carry):
            to = peer(i)
            pltpu.make_async_remote_copy(
                src_ref=src.at[c, at(to * per, per)],
                dst_ref=dst.at[c, at(ep * per, per)],
                send_sem=ssem.at[c], recv_sem=rsem.at[c],
                device_id={"ep": to}, device_id_type=MESH,
            ).start()
            return carry

        lax.fori_loop(1, n_ep, one, 0)
        local_rows(c, src, dst, dls if src is tx and dst is rx else rls).start()

    def all_but_one(ref, c, sem):
        some = ref.at[c, pl.ds(0, rows - per)]
        pltpu.make_async_copy(some, some, sem.at[c]).wait()

    def project(who):
        r = at(who * seg, seg)

        def one(n, carry):
            cols = at(n * 256, 256)
            pj[r, cols] = jnp.dot(na[r, :], wa[:, cols], preferred_element_type=F32).astype(BF16)
            return carry

        lax.fori_loop(0, (3 * kw + 2 * vw) // 256, one, 0)

    for c in range(CHUNKS):
        arrived(block(c, left), agr.at[c, 0])
        fwd = block(c, left, 0)
        send_tp(fwd, fwd, ags.at[c, 2], agr.at[c, 2], right)
        arrived(block(c, right), agr.at[c, 1])
        fwd = block(c, right, 1)
        send_tp(fwd, fwd, ags.at[c, 3], agr.at[c, 3], left)
        attention_send(c)
        arrived(block(c, across, 0), agr.at[c, 2])
        arrived(block(c, across, 1), agr.at[c, 3])

        def build(t, carry, c=c):
            r = at(t * part_rows, part_rows)
            tx[c, r, :] = jnp.dot(onehot[r, :], gm[c], preferred_element_type=F32).astype(BF16)
            return carry

        lax.fori_loop(0, rows // part_rows, build, 0)
        spread(c, tx, rx, dts, drs)
        if c == 0:
            for copy in loads[2:7]:
                copy.wait()
            project(tp)

    for i in range(4):
        arrived(ablock(left, i), aar.at[0, i])
        if i < 2:
            fwd = ablock(left, i)
            send_tp(fwd, fwd, aas.at[2, i], aar.at[2, i], right)
        arrived(ablock(right, i), aar.at[1, i])
        if i >= 2:
            fwd = ablock(right, i)
            send_tp(fwd, fwd, aas.at[2, i], aar.at[2, i], left)
    project(left)
    project(right)

    loads[7].wait()
    loads[8].wait()

    def shared(t, carry):
        r = at(t * tok, tok)
        g = jnp.zeros((tok, jv.shape[1]), F32)
        u = jnp.zeros((tok, jv.shape[1]), F32)
        for c in range(CHUNKS):
            xs = gm[c, r, :]
            g = g + jnp.dot(xs, jv[c * wc : (c + 1) * wc, :], preferred_element_type=F32)
            u = u + jnp.dot(xs, ju[c * wc : (c + 1) * wc, :], preferred_element_type=F32)
        shid[r, :] = (jax.nn.silu(g) * u).astype(BF16)
        return carry

    lax.fori_loop(0, n_tp, shared, 0)

    def weights(m, carry):
        both = jnp.concatenate([metas[at(8 * m, 8), :], jnp.zeros((tok - 8, tok), F32)], axis=0).T
        spot = both[:, 0:2].astype(jnp.int32)
        for c in range(rows // 256):
            ids = lax.broadcasted_iota(jnp.int32, (tok, 256), 1) + c * 256
            w = jnp.where(ids == spot[:, 0:1], both[:, 2:3], 0.0) + jnp.where(
                ids == spot[:, 1:2], both[:, 3:4], 0.0
            )
            weigh[at(m * tok, tok), c * 256 : (c + 1) * 256] = w.astype(BF16)
        return carry

    lax.fori_loop(0, n_tp, weights, 0)

    for i in range(4):
        arrived(ablock(across, i), aar.at[2, i])
    project(across)
    late_load = pltpu.make_async_copy(wr_hbm, wa, wsem.at[13])
    late_load.start()

    state[...] = jnp.zeros_like(state)

    def iota(dims, axis):
        return lax.broadcasted_iota(jnp.int32, dims, axis)

    lower = jnp.where(iota((SPAN, SPAN), 0) >= iota((SPAN, SPAN), 1), 1.0, 0.0)
    causal = iota((SPAN, kw), 0) >= lax.rem(iota((SPAN, kw), 1), SPAN)
    head_of = iota((SPAN, kw), 1) // 64
    kmask = jnp.where(iota((kw, kw), 0) // 64 == iota((kw, kw), 1) // 64, 1.0, 0.0).astype(BF16)
    vmask = jnp.where(iota((kw, vw), 0) // 64 == iota((kw, vw), 1) // 128, 1.0, 0.0)
    vmask16 = vmask.astype(BF16)

    def span(n, carry):
        past, past_tall = carry
        r = at(n * SPAN, SPAN)
        q = pj[r, 0:kw].astype(F32) * 0.125
        k = pj[r, kw : 2 * kw].astype(F32)
        z = pj[r, 2 * kw : 3 * kw].astype(F32) + shift_ref[...]
        v = pj[r, 3 * kw : 3 * kw + vw]
        extra = fade_ref[r, :]
        add = extra[:, 0:1]
        for h in range(1, heads):
            add = jnp.where(head_of == h, extra[:, h : h + 1], add)
        rate = (jnp.minimum(z, 0.0) - jnp.log1p(jnp.exp(-jnp.abs(z)))) * 0.0625 + add
        running = jnp.dot(lower, rate, precision=EXACT, preferred_element_type=F32)
        total = running[SPAN - 1 : SPAN]
        qf = q * jnp.exp(running)
        kd = (k * jnp.exp(-running)).astype(BF16)
        ku = (k * jnp.exp(total - running)).astype(BF16)
        qg[r, :] = (qf * jnp.exp(past)).astype(BF16)
        qf = qf.astype(BF16)
        wide_k = jnp.concatenate([kd] * heads, axis=0) * kmask
        scores = lax.dot_general(qf, wide_k, (((1,), (1,)), ((), ())), preferred_element_type=F32)
        scores = jnp.where(causal, scores, 0.0).astype(BF16)
        wide_v = jnp.concatenate([v] * heads, axis=0) * vmask16
        held = state[...]
        att[r, :] = jnp.dot(scores, wide_v, preferred_element_type=F32) + jnp.dot(
            qf, held.astype(BF16), preferred_element_type=F32
        )
        grown = lax.dot_general(ku, v, (((0,), (0,)), ((), ())), preferred_element_type=F32)
        tall_total = lax.dot_general(
            rate, jnp.ones((SPAN, 128), F32), (((0,), (0,)), ((), ())),
            precision=EXACT, preferred_element_type=F32,
        )
        fade = jnp.exp(tall_total)
        state[...] = jnp.concatenate([fade] * heads, axis=1) * held + grown * vmask
        return past + total, past_tall + tall_total

    _, whole = lax.fori_loop(
        0, segrows // SPAN, span, (jnp.zeros((1, kw), F32), jnp.zeros((kw, 128), F32))
    )
    own_fade = jnp.exp(whole)
    own_state = jnp.concatenate(
        [state[64 * h : 64 * h + 64, 128 * h : 128 * h + 128] for h in range(heads)], axis=0
    )

    def put(level, fade, held):
        sent[level, 0] = fade.astype(BF16)
        sent[level, 1] = held.astype(BF16)

    def share(level, slot, to):
        pltpu.make_async_remote_copy(
            src_ref=sent.at[level], dst_ref=heard.at[slot], send_sem=ss.at[slot], recv_sem=sr.at[slot],
            device_id={"ep": to}, device_id_type=MESH,
        ).start()

    def hear(level, slot):
        arrived(heard.at[slot], sr.at[slot])
        pltpu.make_async_copy(sent.at[level], sent.at[level], ss.at[slot]).wait()

    def after(first, second):
        return first[0] * second[0], second[0] * first[1] + second[1]

    def pick(flag, pair, other):
        return tuple(jnp.where(flag, a, b) for a, b in zip(pair, other))

    neutral = (jnp.ones((kw, 128), F32), jnp.zeros((kw, 128), F32))

    def load_pair(slot):
        return heard[slot, 0].astype(F32), heard[slot, 1].astype(F32)

    def ring_fold(base, place, me):
        prefix, everything = neutral, neutral
        rounded = tuple(a.astype(BF16).astype(F32) for a in me)
        for j in range(4):
            there = rounded
            for d in range(1, 4):
                there = pick(lax.rem(place + 4 - d, 4) == j, load_pair(base + d - 1), there)
            everything = after(everything, there)
            prefix = pick(place > j, after(prefix, there), prefix)
        return prefix, everything

    put(0, own_fade, own_state)
    share(0, 0, zz * 8 + yy * 2 + (1 - core))

    def level_one():
        hear(0, 0)
        mate = load_pair(0)
        me = (sent[0, 0].astype(F32), sent[0, 1].astype(F32))
        low, high = pick(core == 0, me, mate), pick(core == 0, mate, me)
        chip = after(low, high)
        put(1, *chip)
        for d in range(1, 4):
            share(1, d, zz * 8 + lax.rem(yy + d, 4) * 2 + core)
        return pick(core == 0, neutral, mate), chip

    def level_two(chip):
        for d in range(1, 4):
            hear(1, d)
        prefix, column = ring_fold(1, yy, chip)
        put(2, *column)
        for d in range(1, 4):
            share(2, 3 + d, lax.rem(zz + d, 4) * 8 + yy * 2 + core)
        return prefix, column

    def level_three(column):
        for d in range(1, 4):
            hear(2, 3 + d)
        return ring_fold(4, zz, column)[0]

    in_chip, chip = level_one()

    for copy in loads[9:11]:
        copy.wait()
    for c in range(CHUNKS):
        local_rows(c, tx, rx, dls).wait()
        all_but_one(rx, c, drs)

    in_column, column = level_two(chip)

    def expert(t, carry):
        r = at(t * part_rows, part_rows)
        late = lax.rem(lax.broadcasted_iota(jnp.int32, (part_rows, ffe), 0) + t * part_rows, 2 * slots) >= slots
        for l in range(2):
            g = jnp.zeros((part_rows, ffe), F32)
            u = jnp.zeros((part_rows, ffe), F32)
            for c in range(CHUNKS):
                xs = rx[c, r, :]
                g = g + jnp.dot(xs, wv[l, c * wc : (c + 1) * wc, :], preferred_element_type=F32)
                u = u + jnp.dot(xs, wu[l, c * wc : (c + 1) * wc, :], preferred_element_type=F32)
            h = jax.nn.silu(g) * u
            h = jnp.where(late, h, 0.0) if l else jnp.where(late, 0.0, h)
            hid[r, l * ffe : (l + 1) * ffe] = h.astype(BF16)
        return carry

    lax.fori_loop(0, rows // part_rows, expert, 0)
    in_slice = level_three(column)
    earlier = after(after(in_slice, in_column), in_chip)

    loads[11].wait()
    for c in range(CHUNKS):
        all_but_one(tx, c, dts)

        def down(t, carry, c=c):
            r = at(t * part_rows, part_rows)
            tx[c, r, :] = jnp.dot(
                hid[r, :], wd[:, c * wc : (c + 1) * wc], preferred_element_type=F32
            ).astype(BF16)
            return carry

        lax.fori_loop(0, rows // part_rows, down, 0)
        spread(c, tx, ry, rts, rrs)

    entering = earlier[1] + earlier[0] * first_ref[...]
    wide_entry = jnp.concatenate([entering.astype(BF16)] * heads, axis=1) * vmask16
    for step in range(n_tp):
        who = lax.rem(tp + step + 1, n_tp)

        def finish(i, carry, who=who):
            r = at(who * seg + i * 128, 128)
            full = att[r, :] + jnp.dot(qg[r, :], wide_entry, preferred_element_type=F32)
            for h in range(heads):
                a = full[:, 128 * h : 128 * h + 128]
                scale = lax.rsqrt(jnp.mean(a * a, axis=-1, keepdims=True) + NORM_EPS)
                g = pj[r, 3 * kw + vw + 128 * h : 3 * kw + vw + 128 * h + 128].astype(F32)
                gain = hgain_ref[:, 128 * h : 128 * h + 128]
                pj[r, 128 * h : 128 * h + 128] = (a * scale * gain * jax.nn.silu(g)).astype(BF16)
            return carry

        lax.fori_loop(0, seg // 128, finish, 0)
        if step < n_tp - 1:
            send_tp(pj.at[at(who * seg, seg), 0:vw], pt.at[step], hs.at[step], hr.at[step], who)

    late_load.wait()
    from_self = pj[at(tp * seg, seg), 0:vw]
    for step in range(n_tp - 1):
        arrived(pt.at[step], hr.at[step])

    def result(n, carry):
        cols = at(n * 512, 512)
        got = jnp.dot(from_self, wa[at(tp * vw, vw), cols], preferred_element_type=F32)
        for step in range(n_tp - 1):
            source = lax.rem(tp + n_tp - step - 1, n_tp)
            got = got + jnp.dot(pt[step], wa[at(source * vw, vw), cols], preferred_element_type=F32)
        mix_out[:, cols] = got.astype(BF16)
        return carry

    lax.fori_loop(0, width // 512, result, 0)

    for copy in sends:
        copy.wait_send()

    loads[12].wait()
    last = []
    for c in range(CHUNKS):
        local_rows(c, tx, ry, rls).wait()
        all_but_one(ry, c, rrs)

        def combine(m, carry, c=c):
            r = at(m * 256, 256)
            got = jnp.dot(weigh[r, :], ry[c], preferred_element_type=F32)
            got = got + jnp.dot(shid[r, :], jd[:, c * wc : (c + 1) * wc], preferred_element_type=F32)
            gm[c, r, :] = got.astype(BF16)
            return carry

        lax.fori_loop(0, n_tp * tok // 256, combine, 0)
        for step in range(1, n_tp):
            to = lax.rem(tp + step, n_tp)
            copy = pltpu.make_async_remote_copy(
                src_ref=gm.at[c, at(to * tok, tok)],
                dst_ref=fx.at[c, step - 1],
                send_sem=fs.at[c, step], recv_sem=fr.at[c, step],
                device_id={"tp": to}, device_id_type=MESH,
            )
            copy.start()
            last.append(copy)

    for c in range(CHUNKS):
        total = gm[c, mine, :].astype(F32)
        for step in range(1, n_tp):
            last[c * (n_tp - 1) + step - 1].wait()
            total = total + fx[c, step - 1].astype(F32)
        moe_out[:, c * wc : (c + 1) * wc] = total.astype(BF16)
        all_but_one(tx, c, rts)


def body(
    xa, ga, wq, wk, wf, wc_, wg, shift, fade, first, hgain, wr,
    x, gain, picked, mixing, wv, wu, wd, jv, ju, jd,
):
    n_ep, n_tp = lax.axis_size("ep"), lax.axis_size("tp")
    tok, width = x.shape
    seg = xa.shape[0]
    kw, vw = wq.shape[1], wc_.shape[1]
    local, _, ffe = wv.shape
    slots = 3 * tok * 2 // (2 * n_ep * local)
    rows = n_ep * n_tp * 2 * slots
    wc = width // CHUNKS
    meta = jnp.concatenate([picked.T.astype(F32), mixing.T, jnp.zeros((4, tok), F32)], axis=0)
    hbm = pl.BlockSpec(memory_space=pl.ANY)
    vmem = pl.BlockSpec(memory_space=pltpu.VMEM)
    dma = pltpu.SemaphoreType.DMA
    V = pltpu.VMEM
    return pl.pallas_call(
        functools.partial(layer_kernel, (n_ep, n_tp, tok, width, slots, ffe, seg, kw, vw)),
        out_shape=(
            jax.ShapeDtypeStruct((seg, width), BF16),
            jax.ShapeDtypeStruct((tok, width), BF16),
        ),
        in_specs=[hbm, vmem] + [hbm] * 5 + [vmem] * 4 + [hbm] + [hbm, vmem, vmem] + [hbm] * 6,
        out_specs=(vmem, vmem),
        scratch_shapes=[
            V((seg, width), BF16),
            V((seg * n_tp, width), BF16),
            V((width, width), BF16),
            V((seg * n_tp, 3 * kw + 2 * vw), BF16),
            V((seg * n_tp, vw), F32),
            V((seg * n_tp, kw), BF16),
            V((kw, vw), F32),
            V((3, 2, kw, 128), BF16),
            V((7, 2, kw, 128), BF16),
            V((n_tp - 1, seg, vw), BF16),
            V((tok, width), BF16), V(wv.shape, BF16), V(wu.shape, BF16), V((2 * ffe, width), BF16),
            V(jv.shape, BF16), V(ju.shape, BF16), V(jd.shape, BF16),
            V((CHUNKS, n_tp * tok, wc), BF16),
            V((8 * n_tp, tok), F32),
            V((rows, n_tp * tok), BF16),
            V((n_tp * tok, rows), BF16),
            V((CHUNKS, rows, wc), BF16),
            V((CHUNKS, rows, wc), BF16),
            V((rows, 2 * ffe), BF16),
            V((CHUNKS, rows, wc), BF16),
            V((n_tp * tok, jv.shape[1]), BF16),
            V((CHUNKS, n_tp - 1, tok, wc), BF16),
            dma((14,)), dma((CHUNKS, 4)), dma((CHUNKS, 4)), dma((n_tp,)), dma((n_tp,)),
            dma((CHUNKS,)), dma((CHUNKS,)), dma((CHUNKS,)),
            dma((CHUNKS,)), dma((CHUNKS,)), dma((CHUNKS,)),
            dma((CHUNKS, n_tp)), dma((CHUNKS, n_tp)),
            dma((3, 4)), dma((3, 4)), dma((7,)), dma((7,)), dma((n_tp,)), dma((n_tp,)),
        ],
        compiler_params=pltpu.CompilerParams(
            collective_id=0, has_side_effects=True, vmem_limit_bytes=67043328
        ),
        name="layer",
    )(
        xa, ga.reshape(1, -1), wq, wk, wf, wc_, wg, shift.reshape(1, -1), fade, first,
        hgain.reshape(1, -1), wr,
        x, gain.reshape(1, -1), meta, wv, wu, wd.reshape(2 * ffe, width), jv, ju, jd,
    )


def solution(mesh):
    return jax.shard_map(
        body,
        mesh=mesh,
        in_specs=(
            P(("ep", "tp"), None),
            P(),
            P(None, "tp"),
            P(None, "tp"),
            P(None, "tp"),
            P(None, "tp"),
            P(None, "tp"),
            P("tp"),
            P("ep", "tp"),
            P("tp", None),
            P("tp"),
            P(),
            P(("ep", "tp"), None),
            P(),
            P(("ep", "tp"), None),
            P(("ep", "tp"), None),
            P("ep", None, "tp"),
            P("ep", None, "tp"),
            P("ep", "tp", None),
            P(None, "tp"),
            P(None, "tp"),
            P("tp", None),
        ),
        out_specs=(P(("ep", "tp"), None), P(("ep", "tp"), None)),
        check_vma=False,
    )
```

```python
import functools
import jax
import jax.numpy as jnp
from jax import lax
from jax.experimental import pallas as pl
from jax.experimental.pallas import tpu as pltpu
from jax.sharding import PartitionSpec as P

NORM_EPS = 1e-06
F32 = jnp.float32
BF16 = jnp.bfloat16
MESH = pl.DeviceIdType.MESH
EXACT = lax.Precision.HIGHEST
CHUNKS = 4
SPAN = 64


def rms(values, gain):
    wide = values.astype(F32)
    scale = lax.rsqrt(jnp.mean(wide * wide, axis=-1, keepdims=True) + NORM_EPS)
    return (wide * scale * gain).astype(BF16)


def at(start, size, unit=None):
    return pl.ds(pl.multiple_of(start, unit or size), size)


def layer_kernel(
    shape,
    xa_hbm, ga_ref, wq_hbm, wk_hbm, wf_hbm, wc_hbm, wg_hbm, shift_ref, fade_ref, first_ref,
    hgain_ref, wr_hbm,
    x_hbm, gain_ref, picks_ref, mixing_ref, wv_hbm, wu_hbm, wd_hbm, jv_hbm, ju_hbm, jd_hbm,
    mix_out, moe_out,
    xa, na, wa, pj, att, qg, state, sent, heard, pt, blocks, fades,
    x_ref, wv, wu, wd, jv, ju, jd,
    gm, metas, onehot, weigh, tx, rx, hid, ry, shid, fx,
    td, rd, rz, xr, xs, zs, fz,
    wsem, ags, agr, ms, mr, dts, drs, dls, rts, rrs, rls, fs, fr,
    aas, aar, ss, sr, hs, hr, nds, ndr, nxs, nxr, ros, ror, rcs, rcr, rzs, rzr, fzs, fzr, nls, hts, hrs, hls, hfs, hfr,
):
    n_ep, n_tp, tok, width, slots, ffe, seg, kw, vw = shape
    per = n_tp * 2 * slots
    rows = n_ep * per
    wc = width // CHUNKS
    sub = wc // n_tp
    part_rows = 512
    heads = vw // 128
    segrows = seg * n_tp
    quarter = seg // 4
    ep = lax.axis_index("ep")
    tp = lax.axis_index("tp")
    core, yy, zz = lax.rem(ep, 2), lax.rem(ep // 2, 4), ep // 8
    right = lax.rem(tp + 1, n_tp)
    left = lax.rem(tp + n_tp - 1, n_tp)
    across = lax.rem(tp + 2, n_tp)

    def peer(i):
        return (
            lax.rem(zz + i // 8, 4) * 8
            + lax.rem(yy + lax.rem(i // 2, 4), 4) * 2
            + lax.rem(core + lax.rem(i, 2), 2)
        )

    pairs = [
        (x_hbm, x_ref), (xa_hbm, xa),
        (wq_hbm, wa.at[:, 0:kw]), (wk_hbm, wa.at[:, kw : 2 * kw]), (wf_hbm, wa.at[:, 2 * kw : 3 * kw]),
        (wc_hbm, wa.at[:, 3 * kw : 3 * kw + vw]), (wg_hbm, wa.at[:, 3 * kw + vw : 3 * kw + 2 * vw]),
        (jv_hbm, jv), (ju_hbm, ju), (wv_hbm, wv), (wu_hbm, wu), (wd_hbm, wd), (jd_hbm, jd),
    ]
    loads = [pltpu.make_async_copy(s, d, wsem.at[i]) for i, (s, d) in enumerate(pairs)]
    for copy in loads:
        copy.start()

    barrier = pltpu.get_barrier_semaphore()

    def greet(i, carry):
        pl.semaphore_signal(barrier, inc=1, device_id={"ep": peer(i)}, device_id_type=MESH)
        return carry

    lax.fori_loop(1, n_ep, greet, 0)
    for step in range(1, n_tp):
        pl.semaphore_signal(
            barrier, inc=1, device_id={"tp": lax.rem(tp + step, n_tp)}, device_id_type=MESH
        )

    loads[0].wait()
    normed = rms(x_ref[...], gain_ref[...])
    mine = at(tp * tok, tok)
    for c in range(CHUNKS):
        gm[c, mine, :] = normed[:, c * wc : (c + 1) * wc]

    meta = jnp.concatenate([picks_ref[...].astype(F32), mixing_ref[...]], axis=0)
    tall = jnp.concatenate([meta, jnp.zeros((tok - 4, tok), F32)], axis=0).T
    before = lax.broadcasted_iota(jnp.int32, (tok, tok), 0) < lax.broadcasted_iota(
        jnp.int32, (tok, tok), 1
    )
    names = meta[0:2].astype(jnp.int32)
    tall_names = tall[:, 0:2].astype(jnp.int32)
    spots = []
    for k in range(2):
        row = names[k : k + 1]
        hits = jnp.zeros((tok, tok), F32)
        for j in range(2):
            hits = hits + jnp.where((tall_names[:, j : j + 1] == row) & before, 1.0, 0.0)
        rank = jnp.sum(hits, axis=0, keepdims=True)
        local = row // 2
        base = (local * per + tp * 2 * slots + (row - 2 * local) * slots).astype(F32)
        spots.append(base + rank)
    metas[at(tp * 8, 8), :] = jnp.concatenate(
        [spots[0], spots[1], meta[2:4], jnp.zeros((4, tok), F32)], axis=0
    )

    pl.semaphore_wait(barrier, n_ep - 1 + n_tp - 1)

    my_meta = metas.at[at(tp * 8, 8)]
    sends = []
    gathers = []

    def send_tp(src, dst, ssem, rsem, to, keep=None):
        copy = pltpu.make_async_remote_copy(
            src_ref=src, dst_ref=dst, send_sem=ssem, recv_sem=rsem,
            device_id={"tp": to}, device_id_type=MESH,
        )
        copy.start()
        (sends if keep is None else keep).append(copy)

    def arrived(ref, sem):
        pltpu.make_async_copy(ref, ref, sem).wait()

    for step in range(1, n_tp):
        send_tp(my_meta, my_meta, ms.at[step], mr.at[step], lax.rem(tp + step, n_tp))

    def block(c, who, half=None):
        if half is None:
            return gm.at[c, at(who * tok, tok)]
        return gm.at[c, at(who * tok + half * (tok // 2), tok // 2)]

    def own_chunk(c):
        own = block(c, tp)
        send_tp(own, own, ags.at[c, 0], agr.at[c, 0], right, gathers)
        send_tp(own, own, ags.at[c, 1], agr.at[c, 1], left, gathers)

    own_chunk(0)
    own_chunk(1)

    loads[1].wait()
    for i in range(4):
        r = slice(i * quarter, (i + 1) * quarter)
        na[at(tp * seg + i * quarter, quarter), :] = rms(xa[r, :], ga_ref[...])

    def ablock(who, i):
        return na.at[at(who * seg + i * quarter, quarter)]

    def attention_send(i):
        own = ablock(tp, i)
        send_tp(own, own, aas.at[0, i], aar.at[0, i], right)
        send_tp(own, own, aas.at[1, i], aar.at[1, i], left)

    def build_tables():
        for step in range(1, n_tp):
            arrived(metas.at[at(lax.rem(tp + n_tp - step, n_tp) * 8, 8)], mr.at[step])

        def table(t, carry):
            r0 = pl.multiple_of(t * 256, 256)
            ids = lax.broadcasted_iota(jnp.int32, (256, tok), 0) + r0
            for m in range(n_tp):
                spot = metas[8 * m : 8 * m + 2, :].astype(jnp.int32)
                hit = (ids == spot[0:1]) | (ids == spot[1:2])
                onehot[pl.ds(r0, 256), m * tok : (m + 1) * tok] = jnp.where(hit, 1.0, 0.0).astype(BF16)
            return carry

        lax.fori_loop(0, rows // 256, table, 0)

    def local_rows(c, src, dst, sem):
        own = at(ep * per, per)
        return pltpu.make_async_copy(src.at[c, own], dst.at[c - 1 if dst is ry else c, own], sem.at[c])

    def spread(c, src, dst, ssem, rsem):
        def one(i, carry):
            to = peer(i)
            pltpu.make_async_remote_copy(
                src_ref=src.at[c, at(to * per, per)],
                dst_ref=dst.at[c - 1 if dst is ry else c, at(ep * per, per)],
                send_sem=ssem.at[c], recv_sem=rsem.at[c],
                device_id={"ep": to}, device_id_type=MESH,
            ).start()
            return carry

        lax.fori_loop(1, n_ep, one, 0)
        local_rows(c, src, dst, dls if src is tx and dst is rx else rls).start()

    def narrow_own(src, dst, k):
        own = at(ep * per, per)
        return pltpu.make_async_copy(src.at[own], dst.at[own], nls.at[k])

    def spread_narrow(src, dst, ssem, rsem, k):
        def one(i, carry):
            to = peer(i)
            pltpu.make_async_remote_copy(
                src_ref=src.at[at(to * per, per)],
                dst_ref=dst.at[at(ep * per, per)],
                send_sem=ssem.at[0], recv_sem=rsem.at[0],
                device_id={"ep": to}, device_id_type=MESH,
            ).start()
            return carry

        lax.fori_loop(1, n_ep, one, 0)
        narrow_own(src, dst, k).start()

    def narrow_done(ref, sem):
        some = ref.at[pl.ds(0, rows - per)]
        pltpu.make_async_copy(some, some, sem.at[0]).wait()

    def all_but_one(ref, c, sem):
        some = ref.at[c - 1 if ref is ry else c, pl.ds(0, rows - per)]
        pltpu.make_async_copy(some, some, sem.at[c]).wait()

    def project(who):
        r = at(who * seg, seg)

        def one(n, carry):
            cols = at(n * 256, 256)
            pj[r, cols] = jnp.dot(na[r, :], wa[:, cols], preferred_element_type=F32).astype(BF16)
            return carry

        lax.fori_loop(0, (3 * kw + 2 * vw) // 256, one, 0)

    def after(first, second):
        return first[0] * second[0], second[0] * first[1] + second[1]

    neutral = (jnp.ones((kw, 128), F32), jnp.zeros((kw, 128), F32))

    def iota(dims, axis):
        return lax.broadcasted_iota(jnp.int32, dims, axis)

    lower = jnp.where(iota((SPAN, SPAN), 0) >= iota((SPAN, SPAN), 1), 1.0, 0.0)
    causal = iota((SPAN, kw), 0) >= lax.rem(iota((SPAN, kw), 1), SPAN)
    head_of = iota((SPAN, kw), 1) // 64
    kmask = jnp.where(iota((kw, kw), 0) // 64 == iota((kw, kw), 1) // 64, 1.0, 0.0).astype(BF16)
    vmask = jnp.where(iota((kw, vw), 0) // 64 == iota((kw, vw), 1) // 128, 1.0, 0.0)
    vmask16 = vmask.astype(BF16)

    def span(n, carry):
        past, past_tall = carry
        r = at(n * SPAN, SPAN)
        q = pj[r, 0:kw].astype(F32) * 0.125
        k = pj[r, kw : 2 * kw].astype(F32)
        z = pj[r, 2 * kw : 3 * kw].astype(F32) + shift_ref[...]
        v = pj[r, 3 * kw : 3 * kw + vw]
        extra = fades[r, :]
        add = extra[:, 0:1]
        for h in range(1, heads):
            add = jnp.where(head_of == h, extra[:, h : h + 1], add)
        rate = (jnp.minimum(z, 0.0) - jnp.log1p(jnp.exp(-jnp.abs(z)))) * 0.0625 + add
        running = jnp.dot(lower, rate, precision=EXACT, preferred_element_type=F32)
        total = running[SPAN - 1 : SPAN]
        qf = q * jnp.exp(running)
        kd = (k * jnp.exp(-running)).astype(BF16)
        ku = (k * jnp.exp(total - running)).astype(BF16)
        qg[r, :] = (qf * jnp.exp(past)).astype(BF16)
        qf = qf.astype(BF16)
        wide_k = jnp.concatenate([kd] * heads, axis=0) * kmask
        scores = lax.dot_general(qf, wide_k, (((1,), (1,)), ((), ())), preferred_element_type=F32)
        scores = jnp.where(causal, scores, 0.0).astype(BF16)
        wide_v = jnp.concatenate([v] * heads, axis=0) * vmask16
        held = state[...]
        att[r, :] = jnp.dot(scores, wide_v, preferred_element_type=F32) + jnp.dot(
            qf, held.astype(BF16), preferred_element_type=F32
        )
        grown = lax.dot_general(ku, v, (((0,), (0,)), ((), ())), preferred_element_type=F32)
        tall_total = lax.dot_general(
            rate, jnp.ones((SPAN, 128), F32), (((0,), (0,)), ((), ())),
            precision=EXACT, preferred_element_type=F32,
        )
        fade = jnp.exp(tall_total)
        state[...] = jnp.concatenate([fade] * heads, axis=1) * held + grown * vmask
        return past + total, past_tall + tall_total

    def spans(who):
        state[...] = jnp.zeros_like(state)
        first = who * (seg // SPAN)
        _, tall_log = lax.fori_loop(
            0, seg // SPAN, lambda n, carry: span(first + n, carry),
            (jnp.zeros((1, kw), F32), jnp.zeros((kw, 128), F32)),
        )
        blocks[who, 0] = jnp.exp(tall_log)
        for h in range(heads):
            blocks[who, 1, 64 * h : 64 * h + 64, :] = state[64 * h : 64 * h + 64, 128 * h : 128 * h + 128]

    def forward(c):
        arrived(block(c, left), agr.at[c, 0])
        fwd = block(c, left, 0)
        send_tp(fwd, fwd, ags.at[c, 2], agr.at[c, 2], right, gathers)
        arrived(block(c, right), agr.at[c, 1])
        fwd = block(c, right, 1)
        send_tp(fwd, fwd, ags.at[c, 3], agr.at[c, 3], left, gathers)

    def dispatch(c):
        arrived(block(c, across, 0), agr.at[c, 2])
        arrived(block(c, across, 1), agr.at[c, 3])

        def build(t, carry):
            r = at(t * part_rows, part_rows)
            tx[c, r, :] = jnp.dot(onehot[r, :], gm[c], preferred_element_type=F32).astype(BF16)
            return carry

        def narrow(t, carry):
            r = at(t * part_rows, part_rows)
            td[r, :] = jnp.dot(
                onehot[r, :], gm[0, :, at(tp * sub, sub)], preferred_element_type=F32
            ).astype(BF16)
            return carry

        if c == 0:
            lax.fori_loop(0, rows // part_rows, narrow, 0)
            spread_narrow(td, rd, nds, ndr, 0)
        else:
            lax.fori_loop(0, rows // part_rows, build, 0)
            spread(c, tx, rx, dts, drs)

    forward(0)
    build_tables()
    forward(1)
    own_chunk(2)
    attention_send(0)
    dispatch(0)
    dispatch(1)
    forward(2)
    attention_send(1)
    own_chunk(3)
    attention_send(2)
    attention_send(3)
    for copy in loads[2:7]:
        copy.wait()
    project(tp)
    dispatch(2)
    for m in range(n_tp * seg // 128):
        wide = jnp.concatenate([fade_ref[:, 128 * m : 128 * m + 128], jnp.zeros((124, 128), F32)], axis=0)
        fades[128 * m : 128 * m + 128, :] = wide.T
    spans(tp)
    forward(3)
    for i in range(4):
        arrived(ablock(left, i), aar.at[0, i])
        if i < 2:
            fwd = ablock(left, i)
            send_tp(fwd, fwd, aas.at[2, i], aar.at[2, i], right)
        arrived(ablock(right, i), aar.at[1, i])
        if i >= 2:
            fwd = ablock(right, i)
            send_tp(fwd, fwd, aas.at[2, i], aar.at[2, i], left)
    narrow_own(td, rd, 0).wait()
    narrow_done(rd, ndr)
    my_slice = rx.at[0, :, at(tp * sub, sub)]
    for step in range(1, n_tp):
        send_tp(rd, my_slice, nxs.at[step], nxr.at[step], lax.rem(tp + step, n_tp))
    keep = pltpu.make_async_copy(rd, my_slice, nls.at[1])
    keep.start()
    dispatch(3)
    project(left)
    project(right)
    spans(left)
    spans(right)
    for i in range(4):
        arrived(ablock(across, i), aar.at[2, i])
    project(across)
    spans(across)
    late_load = pltpu.make_async_copy(wr_hbm, wa, wsem.at[13])
    late_load.start()
    whole = neutral
    for m in range(n_tp):
        whole = after(whole, (blocks[m, 0], blocks[m, 1]))
    own_fade, own_state = whole

    def put(level, fade, held):
        rows_of = [fade[128 * i : 128 * i + 128].T[0:8] for i in range(kw // 128)]
        flat = jnp.concatenate([rows_of[0][0:1], rows_of[1][0:1], jnp.zeros((14, 128), F32)], axis=0)
        sent[level, 0:kw] = held.astype(BF16)
        sent[level, kw : kw + 16] = flat.astype(BF16)

    def share(level, slot, to):
        pltpu.make_async_remote_copy(
            src_ref=sent.at[level], dst_ref=heard.at[slot], send_sem=ss.at[slot], recv_sem=sr.at[slot],
            device_id={"ep": to}, device_id_type=MESH,
        ).start()

    def hear(level, slot):
        arrived(heard.at[slot], sr.at[slot])
        pltpu.make_async_copy(sent.at[level], sent.at[level], ss.at[slot]).wait()

    def pick(flag, pair, other):
        return tuple(jnp.where(flag, a, b) for a, b in zip(pair, other))

    def load_pair(slot):
        return unpack(heard[slot])

    def unpack(packed):
        flat = packed[kw : kw + 16].astype(F32)
        fade = jnp.concatenate(
            [jnp.broadcast_to(flat[i : i + 1], (128, 128)).T for i in range(kw // 128)], axis=0
        )
        return fade, packed[0:kw].astype(F32)

    def ring_fold(base, place, me):
        prefix, everything = neutral, neutral
        rounded = tuple(a.astype(BF16).astype(F32) for a in me)
        for j in range(4):
            there = rounded
            for d in range(1, 4):
                there = pick(lax.rem(place + 4 - d, 4) == j, load_pair(base + d - 1), there)
            everything = after(everything, there)
            prefix = pick(place > j, after(prefix, there), prefix)
        return prefix, everything

    put(0, own_fade, own_state)
    share(0, 0, zz * 8 + yy * 2 + (1 - core))

    def level_one():
        hear(0, 0)
        mate = load_pair(0)
        me = unpack(sent[0])
        low, high = pick(core == 0, me, mate), pick(core == 0, mate, me)
        chip = after(low, high)
        put(1, *chip)
        for d in range(1, 4):
            share(1, d, zz * 8 + lax.rem(yy + d, 4) * 2 + core)
        return pick(core == 0, neutral, mate), chip

    def level_two(chip):
        for d in range(1, 4):
            hear(1, d)
        prefix, column = ring_fold(1, yy, chip)
        put(2, *column)
        for d in range(1, 4):
            share(2, 3 + d, lax.rem(zz + d, 4) * 8 + yy * 2 + core)
        return prefix, column

    def level_three(column):
        for d in range(1, 4):
            hear(2, 3 + d)
        return ring_fold(4, zz, column)[0]

    in_chip, chip = level_one()
    loads[7].wait()
    loads[8].wait()

    def shared(t, carry):
        r = at(t * tok, tok)
        g = jnp.zeros((tok, jv.shape[1]), F32)
        u = jnp.zeros((tok, jv.shape[1]), F32)
        for c in range(CHUNKS):
            xs = gm[c, r, :]
            g = g + jnp.dot(xs, jv[c * wc : (c + 1) * wc, :], preferred_element_type=F32)
            u = u + jnp.dot(xs, ju[c * wc : (c + 1) * wc, :], preferred_element_type=F32)
        shid[r, :] = (jax.nn.silu(g) * u).astype(BF16)
        return carry

    lax.fori_loop(0, n_tp, shared, 0)

    for copy in loads[9:11]:
        copy.wait()
    keep.wait()
    for step in range(1, n_tp):
        arrived(rx.at[0, :, at(lax.rem(tp + n_tp - step, n_tp) * sub, sub)], nxr.at[step])
    for c in range(1, CHUNKS):
        local_rows(c, tx, rx, dls).wait()
        all_but_one(rx, c, drs)

    def expert(t, carry):
        r = at(t * part_rows, part_rows)
        late = lax.rem(lax.broadcasted_iota(jnp.int32, (part_rows, ffe), 0) + t * part_rows, 2 * slots) >= slots
        for l in range(2):
            g = jnp.zeros((part_rows, ffe), F32)
            u = jnp.zeros((part_rows, ffe), F32)
            for c in range(CHUNKS):
                xs = rx[c, r, :]
                g = g + jnp.dot(xs, wv[l, c * wc : (c + 1) * wc, :], preferred_element_type=F32)
                u = u + jnp.dot(xs, wu[l, c * wc : (c + 1) * wc, :], preferred_element_type=F32)
            h = jax.nn.silu(g) * u
            h = jnp.where(late, h, 0.0) if l else jnp.where(late, 0.0, h)
            hid[r, l * ffe : (l + 1) * ffe] = h.astype(BF16)
        return carry

    lax.fori_loop(0, rows // part_rows, expert, 0)
    in_column, column = level_two(chip)

    loads[11].wait()
    loads[12].wait()
    narrow_done(td, nds)
    for copy in gathers:
        copy.wait_send()

    def down(c):
        def one(t, carry):
            r = at(t * part_rows, part_rows)
            tx[c, r, :] = jnp.dot(
                hid[r, :], wd[:, c * wc : (c + 1) * wc], preferred_element_type=F32
            ).astype(BF16)
            return carry

        lax.fori_loop(0, rows // part_rows, one, 0)

    all_but_one(tx, 1, dts)
    down(1)
    spread(1, tx, ry, rts, rrs)
    down(0)
    gm[0, :, :] = jnp.dot(shid[...], jd[:, 0:wc], preferred_element_type=F32).astype(BF16)
    for step in range(1, n_tp):
        to = lax.rem(tp + step, n_tp)
        cols = at(to * sub, sub)
        send_tp(tx.at[0, :, cols], xr.at[step - 1], ros.at[step], ror.at[step], to)
        send_tp(gm.at[0, :, cols], xs.at[step - 1], rcs.at[step], rcr.at[step], to)
    all_but_one(tx, 2, dts)
    down(2)
    spread(2, tx, ry, rts, rrs)
    all_but_one(tx, 3, dts)
    down(3)

    def weights(m, carry):
        both = jnp.concatenate([metas[at(8 * m, 8), :], jnp.zeros((tok - 8, tok), F32)], axis=0).T
        spot = both[:, 0:2].astype(jnp.int32)
        for c in range(rows // 256):
            ids = lax.broadcasted_iota(jnp.int32, (tok, 256), 1) + c * 256
            w = jnp.where(ids == spot[:, 0:1], both[:, 2:3], 0.0) + jnp.where(
                ids == spot[:, 1:2], both[:, 3:4], 0.0
            )
            weigh[at(m * tok, tok), c * 256 : (c + 1) * 256] = w.astype(BF16)
        return carry

    lax.fori_loop(0, n_tp, weights, 0)

    in_slice = level_three(column)
    earlier = after(after(in_slice, in_column), in_chip)

    entering = earlier[1] + earlier[0] * first_ref[...]
    for m in range(n_tp):
        fade, held = blocks[m, 0], blocks[m, 1]
        blocks[m, 1] = entering
        entering = fade * entering + held

    for step in range(n_tp):
        who = lax.rem(tp + step + 1, n_tp)
        wide_entry = jnp.concatenate([blocks[who, 1].astype(BF16)] * heads, axis=1) * vmask16

        def finish(i, carry, who=who, wide_entry=wide_entry):
            r = at(who * seg + i * 128, 128)
            full = att[r, :] + jnp.dot(qg[r, :], wide_entry, preferred_element_type=F32)
            for h in range(heads):
                a = full[:, 128 * h : 128 * h + 128]
                scale = lax.rsqrt(jnp.mean(a * a, axis=-1, keepdims=True) + NORM_EPS)
                g = pj[r, 3 * kw + vw + 128 * h : 3 * kw + vw + 128 * h + 128].astype(F32)
                gain = hgain_ref[:, 128 * h : 128 * h + 128]
                pj[r, 128 * h : 128 * h + 128] = (a * scale * gain * jax.nn.silu(g)).astype(BF16)
            return carry

        lax.fori_loop(0, seg // 128, finish, 0)
        if step < n_tp - 1:
            send_tp(pj.at[at(who * seg, seg), 0:vw], pt.at[step], hs.at[step], hr.at[step], who)

    last = []

    def collect(c):
        local_rows(c, tx, ry, rls).wait()
        all_but_one(ry, c, rrs)

        def combine(m, carry, c=c):
            r = at(m * 256, 256)
            got = jnp.dot(weigh[r, :], ry[c - 1], preferred_element_type=F32)
            got = got + jnp.dot(shid[r, :], jd[:, c * wc : (c + 1) * wc], preferred_element_type=F32)
            gm[c, r, :] = got.astype(BF16)
            return carry

        lax.fori_loop(0, n_tp * tok // 256, combine, 0)
        for step in range(1, n_tp):
            to = lax.rem(tp + step, n_tp)
            copy = pltpu.make_async_remote_copy(
                src_ref=gm.at[c, at(to * tok, tok)],
                dst_ref=fx.at[c - 1, step - 1],
                send_sem=fs.at[c, step], recv_sem=fr.at[c, step],
                device_id={"tp": to}, device_id_type=MESH,
            )
            copy.start()
            last.append(copy)

    collect(1)
    for step in range(1, n_tp):
        arrived(xr.at[step - 1], ror.at[step])
        arrived(xs.at[step - 1], rcr.at[step])

    def slices(t, carry):
        r = at(t * 256, 256)
        got = tx[0, r, at(tp * sub, sub)].astype(F32)
        for step in range(n_tp - 1):
            got = got + xr[step, r, :].astype(F32)
        td[r, :] = got.astype(BF16)
        return carry

    lax.fori_loop(0, rows // 256, slices, 0)
    spread_narrow(td, rz, rzs, rzr, 2)
    hc = wc // 2

    def spread_half(k):
        cols = pl.ds(k * hc, hc)

        def one(i, carry):
            to = peer(i)
            pltpu.make_async_remote_copy(
                src_ref=tx.at[3, at(to * per, per), cols],
                dst_ref=ry.at[2, at(ep * per, per), cols],
                send_sem=hts.at[k], recv_sem=hrs.at[k],
                device_id={"ep": to}, device_id_type=MESH,
            ).start()
            return carry

        lax.fori_loop(1, n_ep, one, 0)
        half_own(k).start()

    def half_own(k):
        own, cols = at(ep * per, per), pl.ds(k * hc, hc)
        return pltpu.make_async_copy(tx.at[3, own, cols], ry.at[2, own, cols], hls.at[k])

    def half_done(ref, k, sem):
        some = ref.at[pl.ds(0, rows - per), pl.ds(k * hc, hc)]
        pltpu.make_async_copy(some, some, sem.at[k]).wait()

    spread_half(0)
    spread_half(1)
    collect(2)
    late_load.wait()
    from_self = pj[at(tp * seg, seg), 0:vw]
    for step in range(n_tp - 1):
        arrived(pt.at[step], hr.at[step])

    def result(n, carry):
        cols = at(n * 512, 512)
        got = jnp.dot(from_self, wa[at(tp * vw, vw), cols], preferred_element_type=F32)
        for step in range(n_tp - 1):
            source = lax.rem(tp + n_tp - step - 1, n_tp)
            got = got + jnp.dot(pt[step], wa[at(source * vw, vw), cols], preferred_element_type=F32)
        mix_out[:, cols] = got.astype(BF16)
        return carry

    lax.fori_loop(0, width // 512, result, 0)

    narrow_own(td, rz, 2).wait()
    narrow_done(rz, rzr)
    for m in range(n_tp):
        r = slice(m * tok, (m + 1) * tok)
        got = jnp.dot(weigh[r, :], rz[...], preferred_element_type=F32)
        got = got + gm[0, r, at(tp * sub, sub)].astype(F32)
        for step in range(n_tp - 1):
            got = got + xs[step, r, :].astype(F32)
        zs[r, :] = got.astype(BF16)
    final = []
    for step in range(1, n_tp):
        to = lax.rem(tp + step, n_tp)
        copy = pltpu.make_async_remote_copy(
            src_ref=zs.at[at(to * tok, tok)], dst_ref=fz.at[step - 1],
            send_sem=fzs.at[step], recv_sem=fzr.at[step],
            device_id={"tp": to}, device_id_type=MESH,
        )
        copy.start()
        final.append(copy)

    halves = []

    def collect_half(k):
        half_own(k).wait()
        half_done(ry.at[2], k, hrs)

        def combine(m, carry):
            r = at(m * 256, 256)
            got = jnp.dot(weigh[r, :], ry[2, :, k * hc : (k + 1) * hc], preferred_element_type=F32)
            got = got + jnp.dot(
                shid[r, :], jd[:, 3 * wc + k * hc : 3 * wc + (k + 1) * hc], preferred_element_type=F32
            )
            gm[3, r, k * hc : (k + 1) * hc] = got.astype(BF16)
            return carry

        lax.fori_loop(0, n_tp * tok // 256, combine, 0)
        for step in range(1, n_tp):
            to = lax.rem(tp + step, n_tp)
            copy = pltpu.make_async_remote_copy(
                src_ref=gm.at[3, at(to * tok, tok), pl.ds(k * hc, hc)],
                dst_ref=fx.at[2, step - 1, :, pl.ds(k * hc, hc)],
                send_sem=hfs.at[k, step], recv_sem=hfr.at[k, step],
                device_id={"tp": to}, device_id_type=MESH,
            )
            copy.start()
            halves.append(copy)

    collect_half(0)
    for c in range(1, CHUNKS - 1):
        total = gm[c, mine, :].astype(F32)
        for step in range(1, n_tp):
            last[(c - 1) * (n_tp - 1) + step - 1].wait()
            total = total + fx[c - 1, step - 1].astype(F32)
        moe_out[:, c * wc : (c + 1) * wc] = total.astype(BF16)
        all_but_one(tx, c, rts)
    moe_out[:, at(tp * sub, sub)] = zs[mine, :]
    narrow_done(td, rzs)
    for step in range(1, n_tp):
        final[step - 1].wait()
        moe_out[:, at(lax.rem(tp + n_tp - step, n_tp) * sub, sub)] = fz[step - 1]
    collect_half(1)
    for copy in sends:
        copy.wait_send()

    for k in range(2):
        cols = slice(k * hc, (k + 1) * hc)
        total = gm[3, mine, cols].astype(F32)
        for step in range(1, n_tp):
            halves[k * (n_tp - 1) + step - 1].wait()
            total = total + fx[2, step - 1, :, cols].astype(F32)
        moe_out[:, 3 * wc + k * hc : 3 * wc + (k + 1) * hc] = total.astype(BF16)
        half_done(tx.at[3], k, hts)


def body(
    xa, ga, wq, wk, wf, wc_, wg, shift, fade, first, hgain, wr,
    x, gain, picked, mixing, wv, wu, wd, jv, ju, jd,
):
    n_ep, n_tp = lax.axis_size("ep"), lax.axis_size("tp")
    tok, width = x.shape
    seg = xa.shape[0]
    kw, vw = wq.shape[1], wc_.shape[1]
    local, _, ffe = wv.shape
    slots = 3 * tok * 2 // (2 * n_ep * local)
    rows = n_ep * n_tp * 2 * slots
    wc = width // CHUNKS
    sub = wc // n_tp
    hbm = pl.BlockSpec(memory_space=pl.ANY)
    vmem = pl.BlockSpec(memory_space=pltpu.VMEM)
    dma = pltpu.SemaphoreType.DMA
    V = pltpu.VMEM
    return pl.pallas_call(
        functools.partial(layer_kernel, (n_ep, n_tp, tok, width, slots, ffe, seg, kw, vw)),
        out_shape=(
            jax.ShapeDtypeStruct((seg, width), BF16),
            jax.ShapeDtypeStruct((tok, width), BF16),
        ),
        in_specs=[hbm, vmem] + [hbm] * 5 + [vmem] * 4 + [hbm] + [hbm, vmem, vmem, vmem] + [hbm] * 6,
        out_specs=(vmem, vmem),
        scratch_shapes=[
            V((seg, width), BF16),
            V((seg * n_tp, width), BF16),
            V((width, width), BF16),
            V((seg * n_tp, 3 * kw + 2 * vw), BF16),
            V((seg * n_tp, vw), F32),
            V((seg * n_tp, kw), BF16),
            V((kw, vw), F32),
            V((3, kw + 16, 128), BF16),
            V((7, kw + 16, 128), BF16),
            V((n_tp - 1, seg, vw), BF16),
            V((n_tp, 2, kw, 128), F32),
            V((seg * n_tp, 128), F32),
            V((tok, width), BF16), V(wv.shape, BF16), V(wu.shape, BF16), V((2 * ffe, width), BF16),
            V(jv.shape, BF16), V(ju.shape, BF16), V(jd.shape, BF16),
            V((CHUNKS, n_tp * tok, wc), BF16),
            V((8 * n_tp, tok), F32),
            V((rows, n_tp * tok), BF16),
            V((n_tp * tok, rows), BF16),
            V((CHUNKS, rows, wc), BF16),
            V((CHUNKS, rows, wc), BF16),
            V((rows, 2 * ffe), BF16),
            V((CHUNKS - 1, rows, wc), BF16),
            V((n_tp * tok, jv.shape[1]), BF16),
            V((CHUNKS - 1, n_tp - 1, tok, wc), BF16),
            V((rows, sub), BF16), V((rows, sub), BF16), V((rows, sub), BF16),
            V((n_tp - 1, rows, sub), BF16), V((n_tp - 1, n_tp * tok, sub), BF16),
            V((n_tp * tok, sub), BF16), V((n_tp - 1, tok, sub), BF16),
            dma((14,)), dma((CHUNKS, 4)), dma((CHUNKS, 4)), dma((n_tp,)), dma((n_tp,)),
            dma((CHUNKS,)), dma((CHUNKS,)), dma((CHUNKS,)),
            dma((CHUNKS,)), dma((CHUNKS,)), dma((CHUNKS,)),
            dma((CHUNKS, n_tp)), dma((CHUNKS, n_tp)),
            dma((3, 4)), dma((3, 4)), dma((7,)), dma((7,)), dma((n_tp,)), dma((n_tp,)),
            dma((1,)), dma((1,)), dma((n_tp,)), dma((n_tp,)), dma((n_tp,)), dma((n_tp,)), dma((n_tp,)), dma((n_tp,)),
            dma((1,)), dma((1,)), dma((n_tp,)), dma((n_tp,)), dma((3,)),
            dma((2,)), dma((2,)), dma((2,)), dma((2, n_tp)), dma((2, n_tp)),
        ],
        compiler_params=pltpu.CompilerParams(
            collective_id=0, has_side_effects=True, vmem_limit_bytes=67043328
        ),
        name="layer",
    )(
        xa, ga.reshape(1, -1), wq, wk, wf, wc_, wg, shift.reshape(1, -1), fade.T, first,
        hgain.reshape(1, -1), wr,
        x, gain.reshape(1, -1), picked.T, mixing.T, wv, wu, wd.reshape(2 * ffe, width), jv, ju, jd,
    )


def solution(mesh):
    return jax.shard_map(
        body,
        mesh=mesh,
        in_specs=(
            P(("ep", "tp"), None),
            P(),
            P(None, "tp"),
            P(None, "tp"),
            P(None, "tp"),
            P(None, "tp"),
            P(None, "tp"),
            P("tp"),
            P("ep", "tp"),
            P("tp", None),
            P("tp"),
            P(),
            P(("ep", "tp"), None),
            P(),
            P(("ep", "tp"), None),
            P(("ep", "tp"), None),
            P("ep", None, "tp"),
            P("ep", None, "tp"),
            P("ep", "tp", None),
            P(None, "tp"),
            P(None, "tp"),
            P("tp", None),
        ),
        out_specs=(P(("ep", "tp"), None), P(("ep", "tp"), None)),
        check_vma=False,
    )
```

```python
import functools
import jax
import jax.numpy as jnp
from jax import lax
from jax.experimental import pallas as pl
from jax.experimental.pallas import tpu as pltpu
from jax.sharding import PartitionSpec as P

NORM_EPS = 1e-06
F32 = jnp.float32
BF16 = jnp.bfloat16
MESH = pl.DeviceIdType.MESH
EXACT = lax.Precision.HIGHEST
CHUNKS = 4
SPAN = 64


def rms(values, gain):
    wide = values.astype(F32)
    scale = lax.rsqrt(jnp.mean(wide * wide, axis=-1, keepdims=True) + NORM_EPS)
    return (wide * scale * gain).astype(BF16)


def at(start, size, unit=None):
    return pl.ds(pl.multiple_of(start, unit or size), size)


def layer_kernel(
    shape,
    xa_hbm, ga_ref, wq_hbm, wk_hbm, wf_hbm, wc_hbm, wg_hbm, shift_ref, fade_ref, first_ref,
    hgain_ref, wr_hbm,
    x_hbm, gain_ref, picks_ref, mixing_ref, wv_hbm, wu_hbm, wd_hbm, jv_hbm, ju_hbm, jd_hbm,
    mix_out, moe_out,
    xa, na, wa, pj, att, qg, state, sent, heard, pt, blocks, fades,
    x_ref, wv, wu, wd, jv, ju, jd,
    gm, metas, onehot, weigh, tx, rx, hid, ry, shid, fx,
    td, rd, rz, xr, xs, zs, fz, gs,
    wsem, ags, agr, ms, mr, dts, drs, dls, rts, rrs, rls, fs, fr,
    aas, aar, ss, sr, hs, hr, nds, ndr, nxs, nxr, ros, ror, rcs, rcr, rzs, rzr, fzs, fzr, nls, hts, hrs, hls, hfs, hfr, gss, gsr,
):
    n_ep, n_tp, tok, width, slots, ffe, seg, kw, vw = shape
    per = n_tp * 2 * slots
    rows = n_ep * per
    wc = width // CHUNKS
    sub = wc // n_tp
    part_rows = rows
    heads = vw // 128
    segrows = seg * n_tp
    quarter = seg // 4
    ep = lax.axis_index("ep")
    tp = lax.axis_index("tp")
    core, yy, zz = lax.rem(ep, 2), lax.rem(ep // 2, 4), ep // 8
    right = lax.rem(tp + 1, n_tp)
    left = lax.rem(tp + n_tp - 1, n_tp)
    across = lax.rem(tp + 2, n_tp)

    def peer(i):
        return (
            lax.rem(zz + i // 8, 4) * 8
            + lax.rem(yy + lax.rem(i // 2, 4), 4) * 2
            + lax.rem(core + lax.rem(i, 2), 2)
        )

    def partner(k):
        return peer(lax.rem(k * 11, n_ep))

    def place_there(k):
        i = lax.rem(k * 11, n_ep)
        back = (
            lax.rem(4 - i // 8, 4) * 8 + lax.rem(4 - lax.rem(i // 2, 4), 4) * 2 + lax.rem(i, 2)
        )
        return lax.rem(back * 3, n_ep)

    pairs = [
        (x_hbm, x_ref), (xa_hbm, xa),
        (wq_hbm, wa.at[:, 0:kw]), (wk_hbm, wa.at[:, kw : 2 * kw]), (wf_hbm, wa.at[:, 2 * kw : 3 * kw]),
        (wc_hbm, wa.at[:, 3 * kw : 3 * kw + vw]), (wg_hbm, wa.at[:, 3 * kw + vw : 3 * kw + 2 * vw]),
        (jv_hbm, jv), (ju_hbm, ju), (wv_hbm, wv), (wu_hbm, wu), (wd_hbm, wd), (jd_hbm, jd),
    ]
    loads = [pltpu.make_async_copy(s, d, wsem.at[i]) for i, (s, d) in enumerate(pairs)]
    for copy in loads:
        copy.start()

    barrier = pltpu.get_barrier_semaphore()

    def greet(i, carry):
        pl.semaphore_signal(barrier, inc=1, device_id={"ep": peer(i)}, device_id_type=MESH)
        return carry

    lax.fori_loop(1, n_ep, greet, 0)
    for step in range(1, n_tp):
        pl.semaphore_signal(
            barrier, inc=1, device_id={"tp": lax.rem(tp + step, n_tp)}, device_id_type=MESH
        )

    loads[0].wait()
    normed = rms(x_ref[...], gain_ref[...])
    mine = at(tp * tok, tok)
    for c in range(CHUNKS):
        gm[c, mine, :] = normed[:, c * wc : (c + 1) * wc]

    meta = jnp.concatenate([picks_ref[...].astype(F32), mixing_ref[...]], axis=0)
    tall = jnp.concatenate([meta, jnp.zeros((tok - 4, tok), F32)], axis=0).T
    before = lax.broadcasted_iota(jnp.int32, (tok, tok), 0) < lax.broadcasted_iota(
        jnp.int32, (tok, tok), 1
    )
    names = meta[0:2].astype(jnp.int32)
    tall_names = tall[:, 0:2].astype(jnp.int32)
    spots = []
    for k in range(2):
        row = names[k : k + 1]
        hits = jnp.zeros((tok, tok), F32)
        for j in range(2):
            hits = hits + jnp.where((tall_names[:, j : j + 1] == row) & before, 1.0, 0.0)
        rank = jnp.sum(hits, axis=0, keepdims=True)
        local = row // 2
        base = (local * per + (row - 2 * local) * (n_tp * slots) + tp * slots).astype(F32)
        spots.append(base + rank)
    metas[at(tp * 8, 8), :] = jnp.concatenate(
        [spots[0], spots[1], meta[2:4], jnp.zeros((4, tok), F32)], axis=0
    )

    pl.semaphore_wait(barrier, n_ep - 1 + n_tp - 1)

    my_meta = metas.at[at(tp * 8, 8)]
    sends = []
    gathers = []

    def send_tp(src, dst, ssem, rsem, to, keep=None):
        copy = pltpu.make_async_remote_copy(
            src_ref=src, dst_ref=dst, send_sem=ssem, recv_sem=rsem,
            device_id={"tp": to}, device_id_type=MESH,
        )
        copy.start()
        (sends if keep is None else keep).append(copy)

    def arrived(ref, sem):
        pltpu.make_async_copy(ref, ref, sem).wait()

    for step in range(1, n_tp):
        send_tp(my_meta, my_meta, ms.at[step], mr.at[step], lax.rem(tp + step, n_tp))

    def block(c, who, half=None):
        if half is None:
            return gm.at[c, at(who * tok, tok)]
        return gm.at[c, at(who * tok + half * (tok // 2), tok // 2)]

    def own_chunk(c):
        own = block(c, tp)
        send_tp(own, own, ags.at[c, 0], agr.at[c, 0], right, gathers)
        send_tp(own, own, ags.at[c, 1], agr.at[c, 1], left, gathers)

    gs[mine, :] = gm[0, mine, at(tp * sub, sub)]
    for step in range(1, n_tp):
        to = lax.rem(tp + step, n_tp)
        send_tp(
            gm.at[0, mine, at(to * sub, sub)], gs.at[mine], gss.at[step], gsr.at[step], to, gathers
        )
    own_chunk(1)
    own_chunk(2)

    loads[1].wait()
    for i in range(4):
        r = slice(i * quarter, (i + 1) * quarter)
        na[at(tp * seg + i * quarter, quarter), :] = rms(xa[r, :], ga_ref[...])

    def ablock(who, i):
        return na.at[at(who * seg + i * quarter, quarter)]

    def attention_send(i):
        own = ablock(tp, i)
        send_tp(own, own, aas.at[0, i], aar.at[0, i], right)
        send_tp(own, own, aas.at[1, i], aar.at[1, i], left)

    def build_tables():
        for step in range(1, n_tp):
            arrived(metas.at[at(lax.rem(tp + n_tp - step, n_tp) * 8, 8)], mr.at[step])

        def table(t, carry):
            r0 = pl.multiple_of(t * 256, 256)
            ids = lax.broadcasted_iota(jnp.int32, (256, tok), 0) + r0
            for m in range(n_tp):
                spot = metas[8 * m : 8 * m + 2, :].astype(jnp.int32)
                hit = (ids == spot[0:1]) | (ids == spot[1:2])
                onehot[pl.ds(r0, 256), m * tok : (m + 1) * tok] = jnp.where(hit, 1.0, 0.0).astype(BF16)
            return carry

        lax.fori_loop(0, rows // 256, table, 0)

    def ends(k, out):
        to = partner(k)
        if out:
            return to, at(to * per, per), at(place_there(k) * per, per)
        return to, at(k * per, per), at(ep * per, per)

    def local_rows(c, src, dst, sem):
        out = dst is rx
        own, there = at(ep * per, per), pl.ds(0, per)
        return pltpu.make_async_copy(
            src.at[c, own if out else there], dst.at[c if out else c - 1, there if out else own], sem.at[c]
        )

    def spread(c, src, dst, ssem, rsem):
        out = dst is rx

        def one(k, carry):
            to, here, there = ends(k, out)
            pltpu.make_async_remote_copy(
                src_ref=src.at[c, here],
                dst_ref=dst.at[c if out else c - 1, there],
                send_sem=ssem.at[c], recv_sem=rsem.at[c],
                device_id={"ep": to}, device_id_type=MESH,
            ).start()
            return carry

        lax.fori_loop(1, n_ep, one, 0)
        local_rows(c, src, dst, dls if out else rls).start()

    def narrow_own(src, dst, k):
        own, there = at(ep * per, per), pl.ds(0, per)
        if dst is rd:
            return pltpu.make_async_copy(src.at[own], dst.at[there], nls.at[k])
        return pltpu.make_async_copy(src.at[there], dst.at[own], nls.at[k])

    def spread_narrow(src, dst, ssem, rsem, k):
        def one(i, carry):
            to, here, there = ends(i, dst is rd)
            pltpu.make_async_remote_copy(
                src_ref=src.at[here],
                dst_ref=dst.at[there],
                send_sem=ssem.at[0], recv_sem=rsem.at[0],
                device_id={"ep": to}, device_id_type=MESH,
            ).start()
            return carry

        lax.fori_loop(1, n_ep, one, 0)
        narrow_own(src, dst, k).start()

    def narrow_done(ref, sem):
        some = ref.at[pl.ds(0, rows - per)]
        pltpu.make_async_copy(some, some, sem.at[0]).wait()

    def all_but_one(ref, c, sem):
        some = ref.at[c - 1 if ref is ry else c, pl.ds(0, rows - per)]
        pltpu.make_async_copy(some, some, sem.at[c]).wait()

    def project(who):
        r = at(who * seg, seg)

        for n in range((3 * kw + 2 * vw) // 256):
            cols = slice(n * 256, (n + 1) * 256)
            pj[r, cols] = jnp.dot(na[r, :], wa[:, cols], preferred_element_type=F32).astype(BF16)

    def after(first, second):
        return first[0] * second[0], second[0] * first[1] + second[1]

    neutral = (jnp.ones((kw, 128), F32), jnp.zeros((kw, 128), F32))

    def iota(dims, axis):
        return lax.broadcasted_iota(jnp.int32, dims, axis)

    lower = jnp.where(iota((SPAN, SPAN), 0) >= iota((SPAN, SPAN), 1), 1.0, 0.0)
    causal = iota((SPAN, kw), 0) >= lax.rem(iota((SPAN, kw), 1), SPAN)
    head_of = iota((SPAN, kw), 1) // 64
    kmask = jnp.where(iota((kw, kw), 0) // 64 == iota((kw, kw), 1) // 64, 1.0, 0.0).astype(BF16)
    vmask = jnp.where(iota((kw, vw), 0) // 64 == iota((kw, vw), 1) // 128, 1.0, 0.0)
    vmask16 = vmask.astype(BF16)

    def span(n, carry):
        past, past_tall = carry
        r = at(n * SPAN, SPAN)
        q = pj[r, 0:kw].astype(F32) * 0.125
        k = pj[r, kw : 2 * kw].astype(F32)
        z = pj[r, 2 * kw : 3 * kw].astype(F32) + shift_ref[...]
        v = pj[r, 3 * kw : 3 * kw + vw]
        extra = fades[r, :]
        add = extra[:, 0:1]
        for h in range(1, heads):
            add = jnp.where(head_of == h, extra[:, h : h + 1], add)
        rate = (jnp.minimum(z, 0.0) - jnp.log1p(jnp.exp(-jnp.abs(z)))) * 0.0625 + add
        running = jnp.dot(lower, rate, precision=EXACT, preferred_element_type=F32)
        total = running[SPAN - 1 : SPAN]
        qf = q * jnp.exp(running)
        kd = (k * jnp.exp(-running)).astype(BF16)
        ku = (k * jnp.exp(total - running)).astype(BF16)
        qg[r, :] = (qf * jnp.exp(past)).astype(BF16)
        qf = qf.astype(BF16)
        wide_k = jnp.concatenate([kd] * heads, axis=0) * kmask
        scores = lax.dot_general(qf, wide_k, (((1,), (1,)), ((), ())), preferred_element_type=F32)
        scores = jnp.where(causal, scores, 0.0).astype(BF16)
        wide_v = jnp.concatenate([v] * heads, axis=0) * vmask16
        held = state[...]
        att[r, :] = jnp.dot(scores, wide_v, preferred_element_type=F32) + jnp.dot(
            qf, held.astype(BF16), preferred_element_type=F32
        )
        grown = lax.dot_general(ku, v, (((0,), (0,)), ((), ())), preferred_element_type=F32)
        tall_total = lax.dot_general(
            rate, jnp.ones((SPAN, 128), F32), (((0,), (0,)), ((), ())),
            precision=EXACT, preferred_element_type=F32,
        )
        fade = jnp.exp(tall_total)
        state[...] = jnp.concatenate([fade] * heads, axis=1) * held + grown * vmask
        return past + total, past_tall + tall_total

    def spans(who):
        state[...] = jnp.zeros_like(state)
        first = who * (seg // SPAN)
        _, tall_log = lax.fori_loop(
            0, seg // SPAN, lambda n, carry: span(first + n, carry),
            (jnp.zeros((1, kw), F32), jnp.zeros((kw, 128), F32)), unroll=2,
        )
        blocks[who, 0] = jnp.exp(tall_log)
        for h in range(heads):
            blocks[who, 1, 64 * h : 64 * h + 64, :] = state[64 * h : 64 * h + 64, 128 * h : 128 * h + 128]

    def forward(c):
        arrived(block(c, left), agr.at[c, 0])
        fwd = block(c, left, 0)
        send_tp(fwd, fwd, ags.at[c, 2], agr.at[c, 2], right, gathers)
        arrived(block(c, right), agr.at[c, 1])
        fwd = block(c, right, 1)
        send_tp(fwd, fwd, ags.at[c, 3], agr.at[c, 3], left, gathers)

    def far(c):
        arrived(block(c, across, 0), agr.at[c, 2])
        arrived(block(c, across, 1), agr.at[c, 3])

    def dispatch(c):
        if c == 0:
            for step in range(1, n_tp):
                arrived(gs.at[at(lax.rem(tp + n_tp - step, n_tp) * tok, tok)], gsr.at[step])
        else:
            far(c)

        def build(t, carry):
            r = at(t * part_rows, part_rows)
            tx[c, r, :] = jnp.dot(onehot[r, :], gm[c], preferred_element_type=F32).astype(BF16)
            return carry

        def narrow(t, carry):
            r = at(t * part_rows, part_rows)
            td[r, :] = jnp.dot(
                onehot[r, :], gs[...], preferred_element_type=F32
            ).astype(BF16)
            return carry

        if c == 0:
            lax.fori_loop(0, rows // part_rows, narrow, 0)
            spread_narrow(td, rd, nds, ndr, 0)
        else:
            lax.fori_loop(0, rows // part_rows, build, 0)
            spread(c, tx, rx, dts, drs)

    build_tables()
    dispatch(0)
    forward(1)
    attention_send(0)
    dispatch(1)
    forward(2)
    attention_send(1)
    own_chunk(3)
    attention_send(2)
    attention_send(3)
    for copy in loads[2:7]:
        copy.wait()
    project(tp)
    dispatch(2)
    for m in range(n_tp * seg // 128):
        wide = jnp.concatenate([fade_ref[:, 128 * m : 128 * m + 128], jnp.zeros((124, 128), F32)], axis=0)
        fades[128 * m : 128 * m + 128, :] = wide.T
    spans(tp)
    forward(3)
    for i in range(4):
        arrived(ablock(left, i), aar.at[0, i])
        if i < 2:
            fwd = ablock(left, i)
            send_tp(fwd, fwd, aas.at[2, i], aar.at[2, i], right)
        arrived(ablock(right, i), aar.at[1, i])
        if i >= 2:
            fwd = ablock(right, i)
            send_tp(fwd, fwd, aas.at[2, i], aar.at[2, i], left)
    narrow_own(td, rd, 0).wait()
    narrow_done(rd, ndr)
    my_slice = rx.at[0, :, at(tp * sub, sub)]
    send_tp(rd, my_slice, nxs.at[0], nxr.at[0], right)
    send_tp(rd, my_slice, nxs.at[1], nxr.at[1], left)

    def slice_of(who, half=None):
        cols = at(who * sub, sub)
        if half is None:
            return rx.at[0, :, cols]
        return rx.at[0, pl.ds(half * (rows // 2), rows // 2), cols]

    keep = pltpu.make_async_copy(rd, my_slice, nls.at[1])
    keep.start()
    dispatch(3)
    project(left)
    project(right)
    spans(left)
    spans(right)
    for i in range(4):
        arrived(ablock(across, i), aar.at[2, i])
    project(across)
    spans(across)
    late_load = pltpu.make_async_copy(wr_hbm, wa, wsem.at[13])
    late_load.start()
    arrived(slice_of(left), nxr.at[0])
    fwd = slice_of(left, 0)
    send_tp(fwd, fwd, nxs.at[2], nxr.at[2], right)
    arrived(slice_of(right), nxr.at[1])
    fwd = slice_of(right, 1)
    send_tp(fwd, fwd, nxs.at[3], nxr.at[3], left)
    own_chunk(0)
    whole = neutral
    for m in range(n_tp):
        whole = after(whole, (blocks[m, 0], blocks[m, 1]))
    own_fade, own_state = whole

    def put(level, fade, held):
        rows_of = [fade[128 * i : 128 * i + 128].T[0:8] for i in range(kw // 128)]
        flat = jnp.concatenate([rows_of[0][0:1], rows_of[1][0:1], jnp.zeros((14, 128), F32)], axis=0)
        sent[level, 0:kw] = held.astype(BF16)
        sent[level, kw : kw + 16] = flat.astype(BF16)

    def share(level, slot, to):
        pltpu.make_async_remote_copy(
            src_ref=sent.at[level], dst_ref=heard.at[slot], send_sem=ss.at[slot], recv_sem=sr.at[slot],
            device_id={"ep": to}, device_id_type=MESH,
        ).start()

    def hear(level, slot):
        arrived(heard.at[slot], sr.at[slot])
        pltpu.make_async_copy(sent.at[level], sent.at[level], ss.at[slot]).wait()

    def pick(flag, pair, other):
        return tuple(jnp.where(flag, a, b) for a, b in zip(pair, other))

    def load_pair(slot):
        return unpack(heard[slot])

    def unpack(packed):
        flat = packed[kw : kw + 16].astype(F32)
        fade = jnp.concatenate(
            [jnp.broadcast_to(flat[i : i + 1], (128, 128)).T for i in range(kw // 128)], axis=0
        )
        return fade, packed[0:kw].astype(F32)

    def ring_fold(base, place, me):
        prefix, everything = neutral, neutral
        rounded = tuple(a.astype(BF16).astype(F32) for a in me)
        for j in range(4):
            there = rounded
            for d in range(1, 4):
                there = pick(lax.rem(place + 4 - d, 4) == j, load_pair(base + d - 1), there)
            everything = after(everything, there)
            prefix = pick(place > j, after(prefix, there), prefix)
        return prefix, everything

    put(0, own_fade, own_state)
    share(0, 0, zz * 8 + yy * 2 + (1 - core))

    def level_one():
        hear(0, 0)
        mate = load_pair(0)
        me = unpack(sent[0])
        low, high = pick(core == 0, me, mate), pick(core == 0, mate, me)
        chip = after(low, high)
        put(1, *chip)
        for d in range(1, 4):
            share(1, d, zz * 8 + lax.rem(yy + d, 4) * 2 + core)
        return pick(core == 0, neutral, mate), chip

    def level_two(chip):
        for d in range(1, 4):
            hear(1, d)
        prefix, column = ring_fold(1, yy, chip)
        put(2, *column)
        for d in range(1, 4):
            share(2, 3 + d, lax.rem(zz + d, 4) * 8 + yy * 2 + core)
        return prefix, column

    def level_three(column):
        for d in range(1, 4):
            hear(2, 3 + d)
        return ring_fold(4, zz, column)[0]

    in_chip, chip = level_one()
    for copy in loads[9:11]:
        copy.wait()
    keep.wait()
    arrived(slice_of(across, 0), nxr.at[2])
    arrived(slice_of(across, 1), nxr.at[3])
    for c in range(1, CHUNKS):
        local_rows(c, tx, rx, dls).wait()
        all_but_one(rx, c, drs)

    loads[11].wait()
    loads[12].wait()
    narrow_done(td, nds)

    def down(c):
        def one(t, carry):
            r = at(t * part_rows, part_rows)
            tx[c, r, :] = jnp.dot(
                hid[r, :], wd[:, c * wc : (c + 1) * wc], preferred_element_type=F32
            ).astype(BF16)
            return carry

        lax.fori_loop(0, rows // part_rows, one, 0)

    all_but_one(tx, 1, dts)
    blocks_at_once = 8
    cut = per // 3
    planes = n_ep // blocks_at_once

    def first_return(t, carry):
        r = at(t * blocks_at_once * per, blocks_at_once * per)
        both = []
        for l in range(2):
            g = jnp.zeros((blocks_at_once * 2 * cut, ffe), F32)
            u = jnp.zeros((blocks_at_once * 2 * cut, ffe), F32)
            for c in range(CHUNKS):
                xs = rx[c, r, :].reshape(blocks_at_once, per, wc)[:, l * cut : (l + 2) * cut]
                xs = xs.reshape(blocks_at_once * 2 * cut, wc)
                g = g + jnp.dot(xs, wv[l, c * wc : (c + 1) * wc, :], preferred_element_type=F32)
                u = u + jnp.dot(xs, wu[l, c * wc : (c + 1) * wc, :], preferred_element_type=F32)
            h = jax.nn.silu(g) * u
            ids = lax.rem(lax.broadcasted_iota(jnp.int32, h.shape, 0), 2 * cut)
            h = jnp.where(ids >= per // 2 - cut if l else ids < per // 2, h, 0.0).astype(BF16)
            h = h.reshape(blocks_at_once, 2 * cut, ffe)
            empty = jnp.zeros((blocks_at_once, cut, ffe), BF16)
            h = jnp.concatenate([empty, h] if l else [h, empty], axis=1)
            both.append(h.reshape(blocks_at_once * per, ffe))
        both = jnp.concatenate(both, axis=1)
        hid[r, :] = both
        tx[1, r, :] = jnp.dot(both, wd[:, wc : 2 * wc], preferred_element_type=F32).astype(BF16)

        def one(i, carry):
            k = t * blocks_at_once + i

            @pl.when(k > 0)
            def _():
                to, here, there = ends(k, False)
                pltpu.make_async_remote_copy(
                    src_ref=tx.at[1, here],
                    dst_ref=ry.at[0, there],
                    send_sem=rts.at[1], recv_sem=rrs.at[1],
                    device_id={"ep": to}, device_id_type=MESH,
                ).start()

            return carry

        lax.fori_loop(0, blocks_at_once, one, 0)
        return carry

    in_column, column = level_two(chip)
    lax.fori_loop(0, planes, first_return, 0)
    local_rows(1, tx, ry, rls).start()
    forward(0)

    down(0)
    for step in range(1, n_tp):
        to = lax.rem(tp + step, n_tp)
        cols = at(to * sub, sub)
        send_tp(tx.at[0, :, cols], xr.at[step - 1], ros.at[step], ror.at[step], to)
    all_but_one(tx, 2, dts)
    down(2)
    spread(2, tx, ry, rts, rrs)
    all_but_one(tx, 3, dts)
    down(3)

    def weights(m, carry):
        both = jnp.concatenate([metas[at(8 * m, 8), :], jnp.zeros((tok - 8, tok), F32)], axis=0).T
        spot = both[:, 0:2].astype(jnp.int32)
        for c in range(rows // 256):
            ids = lax.broadcasted_iota(jnp.int32, (tok, 256), 1) + c * 256
            w = jnp.where(ids == spot[:, 0:1], both[:, 2:3], 0.0) + jnp.where(
                ids == spot[:, 1:2], both[:, 3:4], 0.0
            )
            weigh[at(m * tok, tok), c * 256 : (c + 1) * 256] = w.astype(BF16)
        return carry

    lax.fori_loop(0, n_tp, weights, 0)

    in_slice = level_three(column)
    earlier = after(after(in_slice, in_column), in_chip)

    entering = earlier[1] + earlier[0] * first_ref[...]
    for m in range(n_tp):
        fade, held = blocks[m, 0], blocks[m, 1]
        blocks[m, 1] = entering
        entering = fade * entering + held

    for step in range(n_tp):
        who = lax.rem(tp + step + 1, n_tp)
        wide_entry = jnp.concatenate([blocks[who, 1].astype(BF16)] * heads, axis=1) * vmask16

        def finish(i, carry, who=who, wide_entry=wide_entry):
            r = at(who * seg + i * 128, 128)
            full = att[r, :] + jnp.dot(qg[r, :], wide_entry, preferred_element_type=F32)
            for h in range(heads):
                a = full[:, 128 * h : 128 * h + 128]
                scale = lax.rsqrt(jnp.mean(a * a, axis=-1, keepdims=True) + NORM_EPS)
                g = pj[r, 3 * kw + vw + 128 * h : 3 * kw + vw + 128 * h + 128].astype(F32)
                gain = hgain_ref[:, 128 * h : 128 * h + 128]
                pj[r, 128 * h : 128 * h + 128] = (a * scale * gain * jax.nn.silu(g)).astype(BF16)
            return carry

        lax.fori_loop(0, seg // 128, finish, 0)
        if step < n_tp - 1:
            send_tp(pj.at[at(who * seg, seg), 0:vw], pt.at[step], hs.at[step], hr.at[step], who)

    far(0)
    loads[7].wait()
    loads[8].wait()

    def shared(t, carry):
        r = at(t * tok, tok)
        g = jnp.zeros((tok, jv.shape[1]), F32)
        u = jnp.zeros((tok, jv.shape[1]), F32)
        for c in range(CHUNKS):
            xs = gm[c, r, :]
            g = g + jnp.dot(xs, jv[c * wc : (c + 1) * wc, :], preferred_element_type=F32)
            u = u + jnp.dot(xs, ju[c * wc : (c + 1) * wc, :], preferred_element_type=F32)
        shid[r, :] = (jax.nn.silu(g) * u).astype(BF16)
        return carry

    lax.fori_loop(0, n_tp, shared, 0)
    for copy in gathers:
        copy.wait_send()
    gm[0, :, :] = jnp.dot(shid[...], jd[:, 0:wc], preferred_element_type=F32).astype(BF16)
    for step in range(1, n_tp):
        to = lax.rem(tp + step, n_tp)
        send_tp(gm.at[0, :, at(to * sub, sub)], xs.at[step - 1], rcs.at[step], rcr.at[step], to)

    last = []

    def collect(c):
        local_rows(c, tx, ry, rls).wait()
        all_but_one(ry, c, rrs)

        def combine(m, carry, c=c):
            r = at(m * 256, 256)
            got = jnp.dot(weigh[r, :], ry[c - 1], preferred_element_type=F32)
            got = got + jnp.dot(shid[r, :], jd[:, c * wc : (c + 1) * wc], preferred_element_type=F32)
            gm[c, r, :] = got.astype(BF16)
            return carry

        lax.fori_loop(0, n_tp * tok // 256, combine, 0)
        for step in range(1, n_tp):
            to = lax.rem(tp + step, n_tp)
            copy = pltpu.make_async_remote_copy(
                src_ref=gm.at[c, at(to * tok, tok)],
                dst_ref=fx.at[c - 1, step - 1],
                send_sem=fs.at[c, step], recv_sem=fr.at[c, step],
                device_id={"tp": to}, device_id_type=MESH,
            )
            copy.start()
            last.append(copy)

    collect(1)
    for step in range(1, n_tp):
        arrived(xr.at[step - 1], ror.at[step])

    def slices(t, carry):
        r = at(t * 256, 256)
        got = tx[0, r, at(tp * sub, sub)].astype(F32)
        for step in range(n_tp - 1):
            got = got + xr[step, r, :].astype(F32)
        td[r, :] = got.astype(BF16)
        return carry

    lax.fori_loop(0, rows // 256, slices, 0)
    spread_narrow(td, rz, rzs, rzr, 2)
    parts = [(0, wc // 2), (wc // 2, wc // 4), (3 * wc // 4, wc // 4)]

    def spread_half(k):
        cols = pl.ds(*parts[k])

        def one(i, carry):
            to, here, there = ends(i, False)
            pltpu.make_async_remote_copy(
                src_ref=tx.at[3, here, cols],
                dst_ref=ry.at[2, there, cols],
                send_sem=hts.at[k], recv_sem=hrs.at[k],
                device_id={"ep": to}, device_id_type=MESH,
            ).start()
            return carry

        lax.fori_loop(1, n_ep, one, 0)
        half_own(k).start()

    def half_own(k):
        own, cols = at(ep * per, per), pl.ds(*parts[k])
        return pltpu.make_async_copy(tx.at[3, pl.ds(0, per), cols], ry.at[2, own, cols], hls.at[k])

    def half_done(ref, k, sem):
        some = ref.at[pl.ds(0, rows - per), pl.ds(*parts[k])]
        pltpu.make_async_copy(some, some, sem.at[k]).wait()

    for k in range(len(parts)):
        spread_half(k)
    collect(2)
    late_load.wait()
    from_self = pj[at(tp * seg, seg), 0:vw]
    for step in range(n_tp - 1):
        arrived(pt.at[step], hr.at[step])

    def result(n, carry):
        cols = at(n * 512, 512)
        got = jnp.dot(from_self, wa[at(tp * vw, vw), cols], preferred_element_type=F32)
        for step in range(n_tp - 1):
            source = lax.rem(tp + n_tp - step - 1, n_tp)
            got = got + jnp.dot(pt[step], wa[at(source * vw, vw), cols], preferred_element_type=F32)
        mix_out[:, cols] = got.astype(BF16)
        return carry

    lax.fori_loop(0, width // 512, result, 0)

    narrow_own(td, rz, 2).wait()
    narrow_done(rz, rzr)
    for step in range(1, n_tp):
        arrived(xs.at[step - 1], rcr.at[step])
    for m in range(n_tp):
        r = slice(m * tok, (m + 1) * tok)
        got = jnp.dot(weigh[r, :], rz[...], preferred_element_type=F32)
        got = got + gm[0, r, at(tp * sub, sub)].astype(F32)
        for step in range(n_tp - 1):
            got = got + xs[step, r, :].astype(F32)
        zs[r, :] = got.astype(BF16)
    final = []
    for step in range(1, n_tp):
        to = lax.rem(tp + step, n_tp)
        copy = pltpu.make_async_remote_copy(
            src_ref=zs.at[at(to * tok, tok)], dst_ref=fz.at[step - 1],
            send_sem=fzs.at[step], recv_sem=fzr.at[step],
            device_id={"tp": to}, device_id_type=MESH,
        )
        copy.start()
        final.append(copy)

    halves = []

    def collect_half(k):
        half_own(k).wait()
        half_done(ry.at[2], k, hrs)

        start, size = parts[k]

        def combine(m, carry):
            r = at(m * 256, 256)
            got = jnp.dot(weigh[r, :], ry[2, :, start : start + size], preferred_element_type=F32)
            got = got + jnp.dot(
                shid[r, :], jd[:, 3 * wc + start : 3 * wc + start + size], preferred_element_type=F32
            )
            gm[3, r, start : start + size] = got.astype(BF16)
            return carry

        lax.fori_loop(0, n_tp * tok // 256, combine, 0)
        for step in range(1, n_tp):
            to = lax.rem(tp + step, n_tp)
            copy = pltpu.make_async_remote_copy(
                src_ref=gm.at[3, at(to * tok, tok), pl.ds(start, size)],
                dst_ref=fx.at[2, step - 1, :, pl.ds(start, size)],
                send_sem=hfs.at[k, step], recv_sem=hfr.at[k, step],
                device_id={"tp": to}, device_id_type=MESH,
            )
            copy.start()
            halves.append(copy)

    collect_half(0)
    for c in range(1, CHUNKS - 1):
        total = gm[c, mine, :].astype(F32)
        for step in range(1, n_tp):
            last[(c - 1) * (n_tp - 1) + step - 1].wait()
            total = total + fx[c - 1, step - 1].astype(F32)
        moe_out[:, c * wc : (c + 1) * wc] = total.astype(BF16)
        all_but_one(tx, c, rts)
    moe_out[:, at(tp * sub, sub)] = zs[mine, :]
    narrow_done(td, rzs)
    for step in range(1, n_tp):
        final[step - 1].wait()
        moe_out[:, at(lax.rem(tp + n_tp - step, n_tp) * sub, sub)] = fz[step - 1]
    collect_half(1)
    collect_half(2)
    for copy in sends:
        copy.wait_send()

    for k, (start, size) in enumerate(parts):
        cols = slice(start, start + size)
        total = gm[3, mine, cols].astype(F32)
        for step in range(1, n_tp):
            halves[k * (n_tp - 1) + step - 1].wait()
            total = total + fx[2, step - 1, :, cols].astype(F32)
        moe_out[:, 3 * wc + start : 3 * wc + start + size] = total.astype(BF16)
        half_done(tx.at[3], k, hts)


def body(
    xa, ga, wq, wk, wf, wc_, wg, shift, fade, first, hgain, wr,
    x, gain, picked, mixing, wv, wu, wd, jv, ju, jd,
):
    n_ep, n_tp = lax.axis_size("ep"), lax.axis_size("tp")
    tok, width = x.shape
    seg = xa.shape[0]
    kw, vw = wq.shape[1], wc_.shape[1]
    local, _, ffe = wv.shape
    slots = 3 * tok * 2 // (2 * n_ep * local)
    rows = n_ep * n_tp * 2 * slots
    wc = width // CHUNKS
    sub = wc // n_tp
    hbm = pl.BlockSpec(memory_space=pl.ANY)
    vmem = pl.BlockSpec(memory_space=pltpu.VMEM)
    dma = pltpu.SemaphoreType.DMA
    V = pltpu.VMEM
    results = pl.pallas_call(
        functools.partial(layer_kernel, (n_ep, n_tp, tok, width, slots, ffe, seg, kw, vw)),
        out_shape=(
            jax.ShapeDtypeStruct((seg, width), BF16),
            jax.ShapeDtypeStruct((tok, width), BF16),
        ),
        in_specs=[hbm, vmem] + [hbm] * 5 + [vmem] * 4 + [hbm] + [hbm, vmem, vmem, vmem] + [hbm] * 6,
        out_specs=(vmem, vmem),
        scratch_shapes=[
            V((seg, width), BF16),
            V((seg * n_tp, width), BF16),
            V((width, width), BF16),
            V((seg * n_tp, 3 * kw + 2 * vw), BF16),
            V((seg * n_tp, vw), F32),
            V((seg * n_tp, kw), BF16),
            V((kw, vw), F32),
            V((3, kw + 16, 128), BF16),
            V((7, kw + 16, 128), BF16),
            V((n_tp - 1, seg, vw), BF16),
            V((n_tp, 2, kw, 128), F32),
            V((seg * n_tp, 128), F32),
            V((tok, width), BF16), V(wv.shape, BF16), V(wu.shape, BF16), V((2 * ffe, width), BF16),
            V(jv.shape, BF16), V(ju.shape, BF16), V(jd.shape, BF16),
            V((CHUNKS, n_tp * tok, wc), BF16),
            V((8 * n_tp, tok), F32),
            V((rows, n_tp * tok), BF16),
            V((n_tp * tok, rows), BF16),
            V((CHUNKS, rows, wc), BF16),
            V((CHUNKS, rows, wc), BF16),
            V((rows, 2 * ffe), BF16),
            V((CHUNKS - 1, rows, wc), BF16),
            V((n_tp * tok, jv.shape[1]), BF16),
            V((CHUNKS - 1, n_tp - 1, tok, wc), BF16),
            V((rows, sub), BF16), V((rows, sub), BF16), V((rows, sub), BF16),
            V((n_tp - 1, rows, sub), BF16), V((n_tp - 1, n_tp * tok, sub), BF16),
            V((n_tp * tok, sub), BF16), V((n_tp - 1, tok, sub), BF16), V((n_tp * tok, sub), BF16),
            dma((14,)), dma((CHUNKS, 4)), dma((CHUNKS, 4)), dma((n_tp,)), dma((n_tp,)),
            dma((CHUNKS,)), dma((CHUNKS,)), dma((CHUNKS,)),
            dma((CHUNKS,)), dma((CHUNKS,)), dma((CHUNKS,)),
            dma((CHUNKS, n_tp)), dma((CHUNKS, n_tp)),
            dma((3, 4)), dma((3, 4)), dma((7,)), dma((7,)), dma((n_tp,)), dma((n_tp,)),
            dma((1,)), dma((1,)), dma((n_tp,)), dma((n_tp,)), dma((n_tp,)), dma((n_tp,)), dma((n_tp,)), dma((n_tp,)),
            dma((1,)), dma((1,)), dma((n_tp,)), dma((n_tp,)), dma((3,)),
            dma((3,)), dma((3,)), dma((3,)), dma((3, n_tp)), dma((3, n_tp)), dma((n_tp,)), dma((n_tp,)),
        ],
        compiler_params=pltpu.CompilerParams(
            collective_id=0, has_side_effects=True, vmem_limit_bytes=67043328
        ),
        name="layer",
    )(
        xa, ga.reshape(1, -1), wq, wk, wf, wc_, wg, shift.reshape(1, -1), fade.T, first,
        hgain.reshape(1, -1), wr,
        x, gain.reshape(1, -1), picked.T, mixing.T, wv, wu, wd.reshape(2 * ffe, width), jv, ju, jd,
    )
    return pl.pallas_call(
        publish,
        out_shape=tuple(jax.ShapeDtypeStruct(r.shape, r.dtype) for r in results),
        in_specs=[vmem, vmem],
        out_specs=(hbm, hbm),
        scratch_shapes=[dma((2,))],
        name="publish",
    )(*results)


def publish(mix_ref, moe_ref, mix_out, moe_out, sem):
    copies = [
        pltpu.make_async_copy(mix_ref, mix_out, sem.at[0]),
        pltpu.make_async_copy(moe_ref, moe_out, sem.at[1]),
    ]
    for copy in copies:
        copy.start()
    for copy in copies:
        copy.wait()


def solution(mesh):
    return jax.shard_map(
        body,
        mesh=mesh,
        in_specs=(
            P(("ep", "tp"), None),
            P(),
            P(None, "tp"),
            P(None, "tp"),
            P(None, "tp"),
            P(None, "tp"),
            P(None, "tp"),
            P("tp"),
            P("ep", "tp"),
            P("tp", None),
            P("tp"),
            P(),
            P(("ep", "tp"), None),
            P(),
            P(("ep", "tp"), None),
            P(("ep", "tp"), None),
            P("ep", None, "tp"),
            P("ep", None, "tp"),
            P("ep", "tp", None),
            P(None, "tp"),
            P(None, "tp"),
            P("tp", None),
        ),
        out_specs=(P(("ep", "tp"), None), P(("ep", "tp"), None)),
        check_vma=False,
    )
```

```python
import functools
import jax
import jax.numpy as jnp
from jax import lax
from jax.experimental import pallas as pl
from jax.experimental.pallas import tpu as pltpu
from jax.sharding import PartitionSpec as P

NORM_EPS = 1e-06
F32 = jnp.float32
BF16 = jnp.bfloat16
MESH = pl.DeviceIdType.MESH
EXACT = lax.Precision.HIGHEST
CHUNKS = 4
SPAN = 64


def rms(values, gain):
    wide = values.astype(F32)
    scale = lax.rsqrt(jnp.mean(wide * wide, axis=-1, keepdims=True) + NORM_EPS)
    return (wide * scale * gain).astype(BF16)


def at(start, size, unit=None):
    return pl.ds(pl.multiple_of(start, unit or size), size)


def layer_kernel(
    shape,
    xa_hbm, ga_ref, wq_hbm, wk_hbm, wf_hbm, wc_hbm, wg_hbm, shift_ref, fade_ref, first_ref,
    hgain_ref, wr_hbm,
    x_hbm, gain_ref, picks_ref, mixing_ref, wv_hbm, wu_hbm, wd_hbm, jv_hbm, ju_hbm, jd_hbm,
    mix_out, moe_out,
    xa, na, wa, pj, att, qg, state, sent, heard, pt, blocks, fades,
    x_ref, wv, wu, wd, jv, ju, jd,
    gm, metas, onehot, weigh, tx, rx, hid, ry, shid, fx,
    td, rd, rz, xr, xs, zs, fz, gs,
    wsem, ags, agr, ms, mr, dts, drs, dls, rts, rrs, rls, fs, fr,
    aas, aar, ss, sr, hs, hr, nds, ndr, nxs, nxr, ros, ror, rcs, rcr, rzs, rzr, fzs, fzr, nls, hts, hrs, hls, hfs, hfr, gss, gsr,
):
    n_ep, n_tp, tok, width, slots, ffe, seg, kw, vw = shape
    per = n_tp * 2 * slots
    rows = n_ep * per
    wc = width // CHUNKS
    sub = wc // n_tp
    part_rows = rows
    heads = vw // 128
    segrows = seg * n_tp
    quarter = seg // 4
    ep = lax.axis_index("ep")
    tp = lax.axis_index("tp")
    core, yy, zz = lax.rem(ep, 2), lax.rem(ep // 2, 4), ep // 8
    right = lax.rem(tp + 1, n_tp)
    left = lax.rem(tp + n_tp - 1, n_tp)
    across = lax.rem(tp + 2, n_tp)

    def peer(i):
        return (
            lax.rem(zz + i // 8, 4) * 8
            + lax.rem(yy + lax.rem(i // 2, 4), 4) * 2
            + lax.rem(core + lax.rem(i, 2), 2)
        )

    def partner(k):
        return peer(lax.rem(k * 11, n_ep))

    def place_there(k):
        i = lax.rem(k * 11, n_ep)
        back = (
            lax.rem(4 - i // 8, 4) * 8 + lax.rem(4 - lax.rem(i // 2, 4), 4) * 2 + lax.rem(i, 2)
        )
        return lax.rem(back * 3, n_ep)

    pairs = [
        (x_hbm, x_ref), (xa_hbm, xa),
        (wq_hbm, wa.at[:, 0:kw]), (wk_hbm, wa.at[:, kw : 2 * kw]), (wf_hbm, wa.at[:, 2 * kw : 3 * kw]),
        (wc_hbm, wa.at[:, 3 * kw : 3 * kw + vw]), (wg_hbm, wa.at[:, 3 * kw + vw : 3 * kw + 2 * vw]),
        (jv_hbm, jv), (ju_hbm, ju), (wv_hbm, wv), (wu_hbm, wu), (wd_hbm, wd), (jd_hbm, jd),
    ]
    loads = [pltpu.make_async_copy(s, d, wsem.at[i]) for i, (s, d) in enumerate(pairs)]
    for copy in loads:
        copy.start()

    barrier = pltpu.get_barrier_semaphore()

    def greet(i, carry):
        pl.semaphore_signal(barrier, inc=1, device_id={"ep": peer(i)}, device_id_type=MESH)
        return carry

    lax.fori_loop(1, n_ep, greet, 0)
    for step in range(1, n_tp):
        pl.semaphore_signal(
            barrier, inc=1, device_id={"tp": lax.rem(tp + step, n_tp)}, device_id_type=MESH
        )

    loads[0].wait()
    normed = rms(x_ref[...], gain_ref[...])
    mine = at(tp * tok, tok)
    for c in range(CHUNKS):
        gm[c, mine, :] = normed[:, c * wc : (c + 1) * wc]

    meta = jnp.concatenate([picks_ref[...].astype(F32), mixing_ref[...]], axis=0)
    tall = jnp.concatenate([meta, jnp.zeros((tok - 4, tok), F32)], axis=0).T
    before = lax.broadcasted_iota(jnp.int32, (tok, tok), 0) < lax.broadcasted_iota(
        jnp.int32, (tok, tok), 1
    )
    names = meta[0:2].astype(jnp.int32)
    tall_names = tall[:, 0:2].astype(jnp.int32)
    spots = []
    for k in range(2):
        row = names[k : k + 1]
        hits = jnp.zeros((tok, tok), F32)
        for j in range(2):
            hits = hits + jnp.where((tall_names[:, j : j + 1] == row) & before, 1.0, 0.0)
        rank = jnp.sum(hits, axis=0, keepdims=True)
        local = row // 2
        base = (local * per + (row - 2 * local) * (n_tp * slots) + tp * slots).astype(F32)
        spots.append(base + rank)
    metas[at(tp * 8, 8), :] = jnp.concatenate(
        [spots[0], spots[1], meta[2:4], jnp.zeros((4, tok), F32)], axis=0
    )

    pl.semaphore_wait(barrier, n_ep - 1 + n_tp - 1)

    my_meta = metas.at[at(tp * 8, 8)]
    sends = []
    gathers = []

    def send_tp(src, dst, ssem, rsem, to, keep=None):
        copy = pltpu.make_async_remote_copy(
            src_ref=src, dst_ref=dst, send_sem=ssem, recv_sem=rsem,
            device_id={"tp": to}, device_id_type=MESH,
        )
        copy.start()
        (sends if keep is None else keep).append(copy)

    def arrived(ref, sem):
        pltpu.make_async_copy(ref, ref, sem).wait()

    for step in range(1, n_tp):
        send_tp(my_meta, my_meta, ms.at[step], mr.at[step], lax.rem(tp + step, n_tp))

    def block(c, who, half=None):
        if half is None:
            return gm.at[c, at(who * tok, tok)]
        return gm.at[c, at(who * tok + half * (tok // 2), tok // 2)]

    def own_chunk(c):
        own = block(c, tp)
        send_tp(own, own, ags.at[c, 0], agr.at[c, 0], right, gathers)
        send_tp(own, own, ags.at[c, 1], agr.at[c, 1], left, gathers)

    gs[mine, :] = gm[0, mine, at(tp * sub, sub)]
    for step in range(1, n_tp):
        to = lax.rem(tp + step, n_tp)
        send_tp(
            gm.at[0, mine, at(to * sub, sub)], gs.at[mine], gss.at[step], gsr.at[step], to, gathers
        )
    own_chunk(1)
    own_chunk(2)

    loads[1].wait()
    for i in range(4):
        r = slice(i * quarter, (i + 1) * quarter)
        na[at(tp * seg + i * quarter, quarter), :] = rms(xa[r, :], ga_ref[...])

    def ablock(who, i):
        return na.at[at(who * seg + i * quarter, quarter)]

    def attention_send(i):
        own = ablock(tp, i)
        send_tp(own, own, aas.at[0, i], aar.at[0, i], right)
        send_tp(own, own, aas.at[1, i], aar.at[1, i], left)

    def build_tables():
        for step in range(1, n_tp):
            arrived(metas.at[at(lax.rem(tp + n_tp - step, n_tp) * 8, 8)], mr.at[step])

        def table(t, carry):
            r0 = pl.multiple_of(t * 256, 256)
            ids = lax.broadcasted_iota(jnp.int32, (256, tok), 0) + r0
            for m in range(n_tp):
                spot = metas[8 * m : 8 * m + 2, :].astype(jnp.int32)
                hit = (ids == spot[0:1]) | (ids == spot[1:2])
                onehot[pl.ds(r0, 256), m * tok : (m + 1) * tok] = jnp.where(hit, 1.0, 0.0).astype(BF16)
            return carry

        lax.fori_loop(0, rows // 256, table, 0)

    def ends(k, out):
        to = partner(k)
        if out:
            return to, at(to * per, per), at(place_there(k) * per, per)
        return to, at(k * per, per), at(ep * per, per)

    def local_rows(c, src, dst, sem):
        out = dst is rx
        own, there = at(ep * per, per), pl.ds(0, per)
        return pltpu.make_async_copy(
            src.at[c, own if out else there], dst.at[c if out else c - 1, there if out else own], sem.at[c]
        )

    def spread(c, src, dst, ssem, rsem):
        out = dst is rx

        def one(k, carry):
            to, here, there = ends(k, out)
            pltpu.make_async_remote_copy(
                src_ref=src.at[c, here],
                dst_ref=dst.at[c if out else c - 1, there],
                send_sem=ssem.at[c], recv_sem=rsem.at[c],
                device_id={"ep": to}, device_id_type=MESH,
            ).start()
            return carry

        lax.fori_loop(1, n_ep, one, 0)
        local_rows(c, src, dst, dls if out else rls).start()

    def narrow_own(src, dst, k):
        own, there = at(ep * per, per), pl.ds(0, per)
        if dst is rd:
            return pltpu.make_async_copy(src.at[own], dst.at[there], nls.at[k])
        return pltpu.make_async_copy(src.at[there], dst.at[own], nls.at[k])

    def spread_narrow(src, dst, ssem, rsem, k):
        def one(i, carry):
            to, here, there = ends(i, dst is rd)
            pltpu.make_async_remote_copy(
                src_ref=src.at[here],
                dst_ref=dst.at[there],
                send_sem=ssem.at[0], recv_sem=rsem.at[0],
                device_id={"ep": to}, device_id_type=MESH,
            ).start()
            return carry

        lax.fori_loop(1, n_ep, one, 0)
        narrow_own(src, dst, k).start()

    def narrow_done(ref, sem):
        some = ref.at[pl.ds(0, rows - per)]
        pltpu.make_async_copy(some, some, sem.at[0]).wait()

    def all_but_one(ref, c, sem):
        some = ref.at[c - 1 if ref is ry else c, pl.ds(0, rows - per)]
        pltpu.make_async_copy(some, some, sem.at[c]).wait()

    def project(who):
        r = at(who * seg, seg)

        for n in range((3 * kw + 2 * vw) // 256):
            cols = slice(n * 256, (n + 1) * 256)
            pj[r, cols] = jnp.dot(na[r, :], wa[:, cols], preferred_element_type=F32).astype(BF16)

    def after(first, second):
        return first[0] * second[0], second[0] * first[1] + second[1]

    neutral = (jnp.ones((kw, 128), F32), jnp.zeros((kw, 128), F32))

    def iota(dims, axis):
        return lax.broadcasted_iota(jnp.int32, dims, axis)

    lower = jnp.where(iota((SPAN, SPAN), 0) >= iota((SPAN, SPAN), 1), 1.0, 0.0)
    causal = iota((SPAN, kw), 0) >= lax.rem(iota((SPAN, kw), 1), SPAN)
    head_of = iota((SPAN, kw), 1) // 64
    kmask = jnp.where(iota((kw, kw), 0) // 64 == iota((kw, kw), 1) // 64, 1.0, 0.0).astype(BF16)
    vmask = jnp.where(iota((kw, vw), 0) // 64 == iota((kw, vw), 1) // 128, 1.0, 0.0)
    vmask16 = vmask.astype(BF16)

    def span(n, carry):
        past, past_tall = carry
        r = at(n * SPAN, SPAN)
        q = pj[r, 0:kw].astype(F32) * 0.125
        k = pj[r, kw : 2 * kw].astype(F32)
        z = pj[r, 2 * kw : 3 * kw].astype(F32) + shift_ref[...]
        v = pj[r, 3 * kw : 3 * kw + vw]
        extra = fades[r, :]
        add = extra[:, 0:1]
        for h in range(1, heads):
            add = jnp.where(head_of == h, extra[:, h : h + 1], add)
        rate = (jnp.minimum(z, 0.0) - jnp.log1p(jnp.exp(-jnp.abs(z)))) * 0.0625 + add
        running = jnp.dot(lower, rate, precision=EXACT, preferred_element_type=F32)
        total = running[SPAN - 1 : SPAN]
        qf = q * jnp.exp(running)
        kd = (k * jnp.exp(-running)).astype(BF16)
        ku = (k * jnp.exp(total - running)).astype(BF16)
        qg[r, :] = (qf * jnp.exp(past)).astype(BF16)
        qf = qf.astype(BF16)
        wide_k = jnp.concatenate([kd] * heads, axis=0) * kmask
        scores = lax.dot_general(qf, wide_k, (((1,), (1,)), ((), ())), preferred_element_type=F32)
        scores = jnp.where(causal, scores, 0.0).astype(BF16)
        wide_v = jnp.concatenate([v] * heads, axis=0) * vmask16
        held = state[...]
        att[r, :] = jnp.dot(scores, wide_v, preferred_element_type=F32) + jnp.dot(
            qf, held.astype(BF16), preferred_element_type=F32
        )
        grown = lax.dot_general(ku, v, (((0,), (0,)), ((), ())), preferred_element_type=F32)
        tall_total = lax.dot_general(
            rate, jnp.ones((SPAN, 128), F32), (((0,), (0,)), ((), ())),
            precision=EXACT, preferred_element_type=F32,
        )
        fade = jnp.exp(tall_total)
        state[...] = jnp.concatenate([fade] * heads, axis=1) * held + grown * vmask
        return past + total, past_tall + tall_total

    def spans(who):
        state[...] = jnp.zeros_like(state)
        first = who * (seg // SPAN)
        _, tall_log = lax.fori_loop(
            0, seg // SPAN, lambda n, carry: span(first + n, carry),
            (jnp.zeros((1, kw), F32), jnp.zeros((kw, 128), F32)), unroll=2,
        )
        blocks[who, 0] = jnp.exp(tall_log)
        for h in range(heads):
            blocks[who, 1, 64 * h : 64 * h + 64, :] = state[64 * h : 64 * h + 64, 128 * h : 128 * h + 128]

    def forward(c):
        arrived(block(c, left), agr.at[c, 0])
        fwd = block(c, left, 0)
        send_tp(fwd, fwd, ags.at[c, 2], agr.at[c, 2], right, gathers)
        arrived(block(c, right), agr.at[c, 1])
        fwd = block(c, right, 1)
        send_tp(fwd, fwd, ags.at[c, 3], agr.at[c, 3], left, gathers)

    def far(c):
        arrived(block(c, across, 0), agr.at[c, 2])
        arrived(block(c, across, 1), agr.at[c, 3])

    def dispatch(c):
        if c == 0:
            for step in range(1, n_tp):
                arrived(gs.at[at(lax.rem(tp + n_tp - step, n_tp) * tok, tok)], gsr.at[step])
        else:
            far(c)

        def build(t, carry):
            r = at(t * part_rows, part_rows)
            tx[c, r, :] = jnp.dot(onehot[r, :], gm[c], preferred_element_type=F32).astype(BF16)
            return carry

        def narrow(t, carry):
            r = at(t * part_rows, part_rows)
            td[r, :] = jnp.dot(
                onehot[r, :], gs[...], preferred_element_type=F32
            ).astype(BF16)
            return carry

        if c == 0:
            lax.fori_loop(0, rows // part_rows, narrow, 0)
            spread_narrow(td, rd, nds, ndr, 0)
        else:
            lax.fori_loop(0, rows // part_rows, build, 0)
            spread(c, tx, rx, dts, drs)

    build_tables()
    dispatch(0)
    forward(1)
    attention_send(0)
    dispatch(1)
    forward(2)
    attention_send(1)
    own_chunk(3)
    attention_send(2)
    attention_send(3)
    for copy in loads[2:7]:
        copy.wait()
    project(tp)
    dispatch(2)
    for m in range(n_tp * seg // 128):
        wide = jnp.concatenate([fade_ref[:, 128 * m : 128 * m + 128], jnp.zeros((124, 128), F32)], axis=0)
        fades[128 * m : 128 * m + 128, :] = wide.T
    spans(tp)
    forward(3)
    for i in range(4):
        arrived(ablock(left, i), aar.at[0, i])
        if i < 2:
            fwd = ablock(left, i)
            send_tp(fwd, fwd, aas.at[2, i], aar.at[2, i], right)
        arrived(ablock(right, i), aar.at[1, i])
        if i >= 2:
            fwd = ablock(right, i)
            send_tp(fwd, fwd, aas.at[2, i], aar.at[2, i], left)
    narrow_own(td, rd, 0).wait()
    narrow_done(rd, ndr)
    my_slice = rx.at[0, :, at(tp * sub, sub)]
    send_tp(rd, my_slice, nxs.at[0], nxr.at[0], right)
    send_tp(rd, my_slice, nxs.at[1], nxr.at[1], left)

    def slice_of(who, half=None):
        cols = at(who * sub, sub)
        if half is None:
            return rx.at[0, :, cols]
        return rx.at[0, pl.ds(half * (rows // 2), rows // 2), cols]

    keep = pltpu.make_async_copy(rd, my_slice, nls.at[1])
    keep.start()
    dispatch(3)
    project(left)
    project(right)
    spans(left)
    spans(right)
    for i in range(4):
        arrived(ablock(across, i), aar.at[2, i])
    project(across)
    spans(across)
    late_load = pltpu.make_async_copy(wr_hbm, wa, wsem.at[13])
    late_load.start()
    arrived(slice_of(left), nxr.at[0])
    fwd = slice_of(left, 0)
    send_tp(fwd, fwd, nxs.at[2], nxr.at[2], right)
    arrived(slice_of(right), nxr.at[1])
    fwd = slice_of(right, 1)
    send_tp(fwd, fwd, nxs.at[3], nxr.at[3], left)
    own_chunk(0)
    whole = neutral
    for m in range(n_tp):
        whole = after(whole, (blocks[m, 0], blocks[m, 1]))
    own_fade, own_state = whole

    def put(level, fade, held):
        rows_of = [fade[128 * i : 128 * i + 128].T[0:8] for i in range(kw // 128)]
        flat = jnp.concatenate([rows_of[0][0:1], rows_of[1][0:1], jnp.zeros((14, 128), F32)], axis=0)
        sent[level, 0:kw] = held.astype(BF16)
        sent[level, kw : kw + 16] = flat.astype(BF16)

    def share(level, slot, to):
        pltpu.make_async_remote_copy(
            src_ref=sent.at[level], dst_ref=heard.at[slot], send_sem=ss.at[slot], recv_sem=sr.at[slot],
            device_id={"ep": to}, device_id_type=MESH,
        ).start()

    def hear(level, slot):
        arrived(heard.at[slot], sr.at[slot])
        pltpu.make_async_copy(sent.at[level], sent.at[level], ss.at[slot]).wait()

    def pick(flag, pair, other):
        return tuple(jnp.where(flag, a, b) for a, b in zip(pair, other))

    def load_pair(slot):
        return unpack(heard[slot])

    def unpack(packed):
        flat = packed[kw : kw + 16].astype(F32)
        fade = jnp.concatenate(
            [jnp.broadcast_to(flat[i : i + 1], (128, 128)).T for i in range(kw // 128)], axis=0
        )
        return fade, packed[0:kw].astype(F32)

    def ring_fold(base, place, me):
        prefix, everything = neutral, neutral
        rounded = tuple(a.astype(BF16).astype(F32) for a in me)
        for j in range(4):
            there = rounded
            for d in range(1, 4):
                there = pick(lax.rem(place + 4 - d, 4) == j, load_pair(base + d - 1), there)
            everything = after(everything, there)
            prefix = pick(place > j, after(prefix, there), prefix)
        return prefix, everything

    put(0, own_fade, own_state)
    share(0, 0, zz * 8 + yy * 2 + (1 - core))

    def level_one():
        hear(0, 0)
        mate = load_pair(0)
        me = unpack(sent[0])
        low, high = pick(core == 0, me, mate), pick(core == 0, mate, me)
        chip = after(low, high)
        put(1, *chip)
        for d in range(1, 4):
            share(1, d, zz * 8 + lax.rem(yy + d, 4) * 2 + core)
        return pick(core == 0, neutral, mate), chip

    def level_two(chip):
        for d in range(1, 4):
            hear(1, d)
        prefix, column = ring_fold(1, yy, chip)
        put(2, *column)
        for d in range(1, 4):
            share(2, 3 + d, lax.rem(zz + d, 4) * 8 + yy * 2 + core)
        return prefix, column

    def level_three(column):
        for d in range(1, 4):
            hear(2, 3 + d)
        return ring_fold(4, zz, column)[0]

    in_chip, chip = level_one()
    for copy in loads[9:11]:
        copy.wait()
    keep.wait()
    arrived(slice_of(across, 0), nxr.at[2])
    arrived(slice_of(across, 1), nxr.at[3])
    for c in range(1, CHUNKS):
        local_rows(c, tx, rx, dls).wait()
        all_but_one(rx, c, drs)

    loads[11].wait()
    loads[12].wait()
    narrow_done(td, nds)

    def down(c):
        def one(t, carry):
            r = at(t * part_rows, part_rows)
            tx[c, r, :] = jnp.dot(
                hid[r, :], wd[:, c * wc : (c + 1) * wc], preferred_element_type=F32
            ).astype(BF16)
            return carry

        lax.fori_loop(0, rows // part_rows, one, 0)

    all_but_one(tx, 1, dts)
    blocks_at_once = 8
    cut = per // 3
    planes = n_ep // blocks_at_once

    def first_return(t, carry):
        r = at(t * blocks_at_once * per, blocks_at_once * per)
        both = []
        for l in range(2):
            g = jnp.zeros((blocks_at_once * 2 * cut, ffe), F32)
            u = jnp.zeros((blocks_at_once * 2 * cut, ffe), F32)
            for c in range(CHUNKS):
                xs = rx[c, r, :].reshape(blocks_at_once, per, wc)[:, l * cut : (l + 2) * cut]
                xs = xs.reshape(blocks_at_once * 2 * cut, wc)
                g = g + jnp.dot(xs, wv[l, c * wc : (c + 1) * wc, :], preferred_element_type=F32)
                u = u + jnp.dot(xs, wu[l, c * wc : (c + 1) * wc, :], preferred_element_type=F32)
            h = jax.nn.silu(g) * u
            ids = lax.rem(lax.broadcasted_iota(jnp.int32, h.shape, 0), 2 * cut)
            h = jnp.where(ids >= per // 2 - cut if l else ids < per // 2, h, 0.0).astype(BF16)
            h = h.reshape(blocks_at_once, 2 * cut, ffe)
            empty = jnp.zeros((blocks_at_once, cut, ffe), BF16)
            h = jnp.concatenate([empty, h] if l else [h, empty], axis=1)
            both.append(h.reshape(blocks_at_once * per, ffe))
        both = jnp.concatenate(both, axis=1)
        hid[r, :] = both
        tx[1, r, :] = jnp.dot(both, wd[:, wc : 2 * wc], preferred_element_type=F32).astype(BF16)

        def one(i, carry):
            k = t * blocks_at_once + i

            @pl.when(k > 0)
            def _():
                to, here, there = ends(k, False)
                pltpu.make_async_remote_copy(
                    src_ref=tx.at[1, here],
                    dst_ref=ry.at[0, there],
                    send_sem=rts.at[1], recv_sem=rrs.at[1],
                    device_id={"ep": to}, device_id_type=MESH,
                ).start()

            return carry

        lax.fori_loop(0, blocks_at_once, one, 0)
        return carry

    in_column, column = level_two(chip)
    lax.fori_loop(0, planes, first_return, 0)
    local_rows(1, tx, ry, rls).start()
    forward(0)

    down(0)
    for step in range(1, n_tp):
        to = lax.rem(tp + step, n_tp)
        cols = at(to * sub, sub)
        send_tp(tx.at[0, :, cols], xr.at[step - 1], ros.at[step], ror.at[step], to)
    all_but_one(tx, 2, dts)
    down(2)
    spread(2, tx, ry, rts, rrs)
    all_but_one(tx, 3, dts)
    down(3)

    parts = [(0, wc // 2), (wc // 2, wc // 4), (3 * wc // 4, wc // 4)]

    def spread_half(k):
        cols = pl.ds(*parts[k])

        def one(i, carry):
            to, here, there = ends(i, False)
            pltpu.make_async_remote_copy(
                src_ref=tx.at[3, here, cols],
                dst_ref=ry.at[2, there, cols],
                send_sem=hts.at[k], recv_sem=hrs.at[k],
                device_id={"ep": to}, device_id_type=MESH,
            ).start()
            return carry

        lax.fori_loop(1, n_ep, one, 0)
        half_own(k).start()

    def half_own(k):
        own, cols = at(ep * per, per), pl.ds(*parts[k])
        return pltpu.make_async_copy(tx.at[3, pl.ds(0, per), cols], ry.at[2, own, cols], hls.at[k])

    def half_done(ref, k, sem):
        some = ref.at[pl.ds(0, rows - per), pl.ds(*parts[k])]
        pltpu.make_async_copy(some, some, sem.at[k]).wait()

    for k in range(len(parts)):
        spread_half(k)
    def weights(m, carry):
        both = jnp.concatenate([metas[at(8 * m, 8), :], jnp.zeros((tok - 8, tok), F32)], axis=0).T
        spot = both[:, 0:2].astype(jnp.int32)
        for c in range(rows // 256):
            ids = lax.broadcasted_iota(jnp.int32, (tok, 256), 1) + c * 256
            w = jnp.where(ids == spot[:, 0:1], both[:, 2:3], 0.0) + jnp.where(
                ids == spot[:, 1:2], both[:, 3:4], 0.0
            )
            weigh[at(m * tok, tok), c * 256 : (c + 1) * 256] = w.astype(BF16)
        return carry

    lax.fori_loop(0, n_tp, weights, 0)

    in_slice = level_three(column)
    earlier = after(after(in_slice, in_column), in_chip)

    entering = earlier[1] + earlier[0] * first_ref[...]
    for m in range(n_tp):
        fade, held = blocks[m, 0], blocks[m, 1]
        blocks[m, 1] = entering
        entering = fade * entering + held

    for step in range(n_tp):
        who = lax.rem(tp + step + 1, n_tp)
        wide_entry = jnp.concatenate([blocks[who, 1].astype(BF16)] * heads, axis=1) * vmask16

        def finish(i, carry, who=who, wide_entry=wide_entry):
            r = at(who * seg + i * 128, 128)
            full = att[r, :] + jnp.dot(qg[r, :], wide_entry, preferred_element_type=F32)
            for h in range(heads):
                a = full[:, 128 * h : 128 * h + 128]
                scale = lax.rsqrt(jnp.mean(a * a, axis=-1, keepdims=True) + NORM_EPS)
                g = pj[r, 3 * kw + vw + 128 * h : 3 * kw + vw + 128 * h + 128].astype(F32)
                gain = hgain_ref[:, 128 * h : 128 * h + 128]
                pj[r, 128 * h : 128 * h + 128] = (a * scale * gain * jax.nn.silu(g)).astype(BF16)
            return carry

        lax.fori_loop(0, seg // 128, finish, 0)
        if step < n_tp - 1:
            send_tp(pj.at[at(who * seg, seg), 0:vw], pt.at[step], hs.at[step], hr.at[step], who)

    far(0)
    loads[7].wait()
    loads[8].wait()

    def shared(t, carry):
        r = at(t * tok, tok)
        g = jnp.zeros((tok, jv.shape[1]), F32)
        u = jnp.zeros((tok, jv.shape[1]), F32)
        for c in range(CHUNKS):
            xs = gm[c, r, :]
            g = g + jnp.dot(xs, jv[c * wc : (c + 1) * wc, :], preferred_element_type=F32)
            u = u + jnp.dot(xs, ju[c * wc : (c + 1) * wc, :], preferred_element_type=F32)
        shid[r, :] = (jax.nn.silu(g) * u).astype(BF16)
        return carry

    lax.fori_loop(0, n_tp, shared, 0)
    for copy in gathers:
        copy.wait_send()
    gm[0, :, :] = jnp.dot(shid[...], jd[:, 0:wc], preferred_element_type=F32).astype(BF16)
    for step in range(1, n_tp):
        to = lax.rem(tp + step, n_tp)
        send_tp(gm.at[0, :, at(to * sub, sub)], xs.at[step - 1], rcs.at[step], rcr.at[step], to)

    last = []

    def collect(c):
        local_rows(c, tx, ry, rls).wait()
        all_but_one(ry, c, rrs)

        def combine(m, carry, c=c):
            r = at(m * 256, 256)
            got = jnp.dot(weigh[r, :], ry[c - 1], preferred_element_type=F32)
            got = got + jnp.dot(shid[r, :], jd[:, c * wc : (c + 1) * wc], preferred_element_type=F32)
            gm[c, r, :] = got.astype(BF16)
            return carry

        lax.fori_loop(0, n_tp * tok // 256, combine, 0)
        for step in range(1, n_tp):
            to = lax.rem(tp + step, n_tp)
            copy = pltpu.make_async_remote_copy(
                src_ref=gm.at[c, at(to * tok, tok)],
                dst_ref=fx.at[c - 1, step - 1],
                send_sem=fs.at[c, step], recv_sem=fr.at[c, step],
                device_id={"tp": to}, device_id_type=MESH,
            )
            copy.start()
            last.append(copy)

    collect(1)
    for step in range(1, n_tp):
        arrived(xr.at[step - 1], ror.at[step])

    def slices(t, carry):
        r = at(t * 256, 256)
        got = tx[0, r, at(tp * sub, sub)].astype(F32)
        for step in range(n_tp - 1):
            got = got + xr[step, r, :].astype(F32)
        td[r, :] = got.astype(BF16)
        return carry

    lax.fori_loop(0, rows // 256, slices, 0)
    spread_narrow(td, rz, rzs, rzr, 2)
    collect(2)
    late_load.wait()
    from_self = pj[at(tp * seg, seg), 0:vw]
    for step in range(n_tp - 1):
        arrived(pt.at[step], hr.at[step])

    def result(n, carry):
        cols = at(n * 512, 512)
        got = jnp.dot(from_self, wa[at(tp * vw, vw), cols], preferred_element_type=F32)
        for step in range(n_tp - 1):
            source = lax.rem(tp + n_tp - step - 1, n_tp)
            got = got + jnp.dot(pt[step], wa[at(source * vw, vw), cols], preferred_element_type=F32)
        mix_out[:, cols] = got.astype(BF16)
        return carry

    lax.fori_loop(0, width // 512, result, 0)

    narrow_own(td, rz, 2).wait()
    narrow_done(rz, rzr)
    for step in range(1, n_tp):
        arrived(xs.at[step - 1], rcr.at[step])
    for m in range(n_tp):
        r = slice(m * tok, (m + 1) * tok)
        got = jnp.dot(weigh[r, :], rz[...], preferred_element_type=F32)
        got = got + gm[0, r, at(tp * sub, sub)].astype(F32)
        for step in range(n_tp - 1):
            got = got + xs[step, r, :].astype(F32)
        zs[r, :] = got.astype(BF16)
    final = []
    for step in range(1, n_tp):
        to = lax.rem(tp + step, n_tp)
        copy = pltpu.make_async_remote_copy(
            src_ref=zs.at[at(to * tok, tok)], dst_ref=fz.at[step - 1],
            send_sem=fzs.at[step], recv_sem=fzr.at[step],
            device_id={"tp": to}, device_id_type=MESH,
        )
        copy.start()
        final.append(copy)

    halves = []

    def collect_half(k):
        half_own(k).wait()
        half_done(ry.at[2], k, hrs)

        start, size = parts[k]

        def combine(m, carry):
            r = at(m * 256, 256)
            got = jnp.dot(weigh[r, :], ry[2, :, start : start + size], preferred_element_type=F32)
            got = got + jnp.dot(
                shid[r, :], jd[:, 3 * wc + start : 3 * wc + start + size], preferred_element_type=F32
            )
            gm[3, r, start : start + size] = got.astype(BF16)
            return carry

        lax.fori_loop(0, n_tp * tok // 256, combine, 0)
        for step in range(1, n_tp):
            to = lax.rem(tp + step, n_tp)
            copy = pltpu.make_async_remote_copy(
                src_ref=gm.at[3, at(to * tok, tok), pl.ds(start, size)],
                dst_ref=fx.at[2, step - 1, :, pl.ds(start, size)],
                send_sem=hfs.at[k, step], recv_sem=hfr.at[k, step],
                device_id={"tp": to}, device_id_type=MESH,
            )
            copy.start()
            halves.append(copy)

    collect_half(0)
    for c in range(1, CHUNKS - 1):
        total = gm[c, mine, :].astype(F32)
        for step in range(1, n_tp):
            last[(c - 1) * (n_tp - 1) + step - 1].wait()
            total = total + fx[c - 1, step - 1].astype(F32)
        moe_out[:, c * wc : (c + 1) * wc] = total.astype(BF16)
        all_but_one(tx, c, rts)
    moe_out[:, at(tp * sub, sub)] = zs[mine, :]
    narrow_done(td, rzs)
    for step in range(1, n_tp):
        final[step - 1].wait()
        moe_out[:, at(lax.rem(tp + n_tp - step, n_tp) * sub, sub)] = fz[step - 1]
    collect_half(1)
    collect_half(2)
    for copy in sends:
        copy.wait_send()

    for k, (start, size) in enumerate(parts):
        cols = slice(start, start + size)
        total = gm[3, mine, cols].astype(F32)
        for step in range(1, n_tp):
            halves[k * (n_tp - 1) + step - 1].wait()
            total = total + fx[2, step - 1, :, cols].astype(F32)
        moe_out[:, 3 * wc + start : 3 * wc + start + size] = total.astype(BF16)
        half_done(tx.at[3], k, hts)


def body(
    xa, ga, wq, wk, wf, wc_, wg, shift, fade, first, hgain, wr,
    x, gain, picked, mixing, wv, wu, wd, jv, ju, jd,
):
    n_ep, n_tp = lax.axis_size("ep"), lax.axis_size("tp")
    tok, width = x.shape
    seg = xa.shape[0]
    kw, vw = wq.shape[1], wc_.shape[1]
    local, _, ffe = wv.shape
    slots = 3 * tok * 2 // (2 * n_ep * local)
    rows = n_ep * n_tp * 2 * slots
    wc = width // CHUNKS
    sub = wc // n_tp
    hbm = pl.BlockSpec(memory_space=pl.ANY)
    vmem = pl.BlockSpec(memory_space=pltpu.VMEM)
    dma = pltpu.SemaphoreType.DMA
    V = pltpu.VMEM
    results = pl.pallas_call(
        functools.partial(layer_kernel, (n_ep, n_tp, tok, width, slots, ffe, seg, kw, vw)),
        out_shape=(
            jax.ShapeDtypeStruct((seg, width), BF16),
            jax.ShapeDtypeStruct((tok, width), BF16),
        ),
        in_specs=[hbm, vmem] + [hbm] * 5 + [vmem] * 4 + [hbm] + [hbm, vmem, vmem, vmem] + [hbm] * 6,
        out_specs=(vmem, vmem),
        scratch_shapes=[
            V((seg, width), BF16),
            V((seg * n_tp, width), BF16),
            V((width, width), BF16),
            V((seg * n_tp, 3 * kw + 2 * vw), BF16),
            V((seg * n_tp, vw), F32),
            V((seg * n_tp, kw), BF16),
            V((kw, vw), F32),
            V((3, kw + 16, 128), BF16),
            V((7, kw + 16, 128), BF16),
            V((n_tp - 1, seg, vw), BF16),
            V((n_tp, 2, kw, 128), F32),
            V((seg * n_tp, 128), F32),
            V((tok, width), BF16), V(wv.shape, BF16), V(wu.shape, BF16), V((2 * ffe, width), BF16),
            V(jv.shape, BF16), V(ju.shape, BF16), V(jd.shape, BF16),
            V((CHUNKS, n_tp * tok, wc), BF16),
            V((8 * n_tp, tok), F32),
            V((rows, n_tp * tok), BF16),
            V((n_tp * tok, rows), BF16),
            V((CHUNKS, rows, wc), BF16),
            V((CHUNKS, rows, wc), BF16),
            V((rows, 2 * ffe), BF16),
            V((CHUNKS - 1, rows, wc), BF16),
            V((n_tp * tok, jv.shape[1]), BF16),
            V((CHUNKS - 1, n_tp - 1, tok, wc), BF16),
            V((rows, sub), BF16), V((rows, sub), BF16), V((rows, sub), BF16),
            V((n_tp - 1, rows, sub), BF16), V((n_tp - 1, n_tp * tok, sub), BF16),
            V((n_tp * tok, sub), BF16), V((n_tp - 1, tok, sub), BF16), V((n_tp * tok, sub), BF16),
            dma((14,)), dma((CHUNKS, 4)), dma((CHUNKS, 4)), dma((n_tp,)), dma((n_tp,)),
            dma((CHUNKS,)), dma((CHUNKS,)), dma((CHUNKS,)),
            dma((CHUNKS,)), dma((CHUNKS,)), dma((CHUNKS,)),
            dma((CHUNKS, n_tp)), dma((CHUNKS, n_tp)),
            dma((3, 4)), dma((3, 4)), dma((7,)), dma((7,)), dma((n_tp,)), dma((n_tp,)),
            dma((1,)), dma((1,)), dma((n_tp,)), dma((n_tp,)), dma((n_tp,)), dma((n_tp,)), dma((n_tp,)), dma((n_tp,)),
            dma((1,)), dma((1,)), dma((n_tp,)), dma((n_tp,)), dma((3,)),
            dma((3,)), dma((3,)), dma((3,)), dma((3, n_tp)), dma((3, n_tp)), dma((n_tp,)), dma((n_tp,)),
        ],
        compiler_params=pltpu.CompilerParams(
            collective_id=0, has_side_effects=True, vmem_limit_bytes=67043328
        ),
        name="layer",
    )(
        xa, ga.reshape(1, -1), wq, wk, wf, wc_, wg, shift.reshape(1, -1), fade.T, first,
        hgain.reshape(1, -1), wr,
        x, gain.reshape(1, -1), picked.T, mixing.T, wv, wu, wd.reshape(2 * ffe, width), jv, ju, jd,
    )
    return pl.pallas_call(
        publish,
        out_shape=tuple(jax.ShapeDtypeStruct(r.shape, r.dtype) for r in results),
        in_specs=[vmem, vmem],
        out_specs=(hbm, hbm),
        scratch_shapes=[dma((2,))],
        name="publish",
    )(*results)


def publish(mix_ref, moe_ref, mix_out, moe_out, sem):
    copies = [
        pltpu.make_async_copy(mix_ref, mix_out, sem.at[0]),
        pltpu.make_async_copy(moe_ref, moe_out, sem.at[1]),
    ]
    for copy in copies:
        copy.start()
    for copy in copies:
        copy.wait()


def solution(mesh):
    return jax.shard_map(
        body,
        mesh=mesh,
        in_specs=(
            P(("ep", "tp"), None),
            P(),
            P(None, "tp"),
            P(None, "tp"),
            P(None, "tp"),
            P(None, "tp"),
            P(None, "tp"),
            P("tp"),
            P("ep", "tp"),
            P("tp", None),
            P("tp"),
            P(),
            P(("ep", "tp"), None),
            P(),
            P(("ep", "tp"), None),
            P(("ep", "tp"), None),
            P("ep", None, "tp"),
            P("ep", None, "tp"),
            P("ep", "tp", None),
            P(None, "tp"),
            P(None, "tp"),
            P("tp", None),
        ),
        out_specs=(P(("ep", "tp"), None), P(("ep", "tp"), None)),
        check_vma=False,
    )
```
